32 devices in a mesh: ep: 8 (over z, core), tp: 4 (over y, x).
Axes of the slice: x: 2, y: 2, z: 4, core: 2. Of those that a mesh axis runs over, the one named last changes fastest.
Arguments:
- tokens: bfloat16 [2048, 2048], P('ep'), may hold values from -6 to 6
- norm_gain: float32 [2048], replicated, may hold values from 0.1 to 1.9
- route_ids: int32 [2048, 4], P('ep'), may hold values from 0 to 15, all different within a row; in each aligned block of 256 rows (0 to 255, 256 to 511, ...) at most 96 rows name the same one
- route_weights: float32 [2048, 4], P('ep'), may hold values from 0.1 to 1
- w_gate: bfloat16 [16, 2048, 2048], P('ep', None, 'tp'), may hold values from -0.33007812 to 0.33007812
- w_up: bfloat16 [16, 2048, 2048], P('ep', None, 'tp'), may hold values from -0.33007812 to 0.33007812
- w_down: bfloat16 [16, 2048, 2048], P('ep', None, 'tp'), may hold values from -0.026489258 to 0.026489258
Outputs:
- mixed_out: bfloat16 [2048, 2048], P('ep', 'tp')
The draws below stay inside these ranges and needn't reach their ends.
Inputs may be any that keep to these rules, and one draw needn't show every extreme that they name: `route_ids`: each token names 4 different experts. Within the tokens of one index of ep (aligned blocks of 256 tokens) no expert is named more than 96 times, a bound that some block reaches.
All inputs are finite; a program needn't handle non-finite values.
Results may differ from the reference program's by a relative error of at most 0.007.
Values may be sent and summed in bfloat16 or wider, within the bound.
A program may use at most 64 MiB of HBM per device.

```python
import math
import jax
import jax.numpy as jnp
import numpy as np
from jax import lax

D = 2048
FF = 2048
TOP_K = 4
TOK_DEV = 256
EXPERTS = 16
TOKENS = 2048
CAP = 96
N_EP = 8


def block_scale(rng, shape, split, smallest, top_value):
    def one(axis_at, parts):
        heights = jax.random.uniform(jax.random.fold_in(jax.random.fold_in(rng, 6), axis_at), (parts,), jnp.float32, smallest / len(split), top_value / len(split))
        return jnp.repeat(jnp.exp(heights), shape[axis_at] // parts).reshape((-1,) + (1,) * (len(shape) - axis_at - 1))

    level = one(*split[0])
    for cut in split[1:]:
        level = level * one(*cut)
    return level


def assign_block(own_key, own, number, rows, amount, top, reach, lean):
    ranking = jax.random.permutation(own_key, amount)
    crowded, ordinary = load_shares(amount, rows * top, reach, lean, True), load_shares(amount, rows * top, reach, lean, False)
    places = jnp.arange(amount)

    def named(tallies, offset_by):
        used = int((tallies > 0).sum())
        fixed = max(1, used // 4)
        passed = fixed + (places - fixed + offset_by * (used - fixed)) % max(1, amount - fixed)
        return jnp.zeros((amount,), jnp.int32).at[ranking[jnp.where(places < fixed, places, passed)]].set(jnp.asarray(tallies, jnp.int32))

    tallies = jnp.where(number % 4 == 0, named(crowded, number // 4), named(ordinary, number - number // 4 - 1))
    mixed = jax.random.permutation(jax.random.fold_in(own, 3), amount)
    giver, sink = mixed[0:amount // 2 * 2:2], mixed[1:amount // 2 * 2:2]
    room = jnp.minimum(tallies[giver] - 1, reach - tallies[sink]) // 2
    room = jnp.where((giver == ranking[0]) | (sink == ranking[0]) | (tallies[sink] == 0), 0, jnp.maximum(room, 0))
    passed = jax.random.randint(jax.random.fold_in(own, 4), (amount // 2,), 0, 1 << 20) % (room + 1)
    tallies = tallies.at[giver].add(-passed).at[sink].add(passed)
    members = jnp.searchsorted(jnp.cumsum(tallies), jnp.arange(rows * top), side="right").astype(jnp.int32)
    listing = members.reshape(top, rows).T
    listing = listing[jax.random.permutation(jax.random.fold_in(own, 1), rows)]
    offset_by = jax.random.randint(jax.random.fold_in(own, 2), (rows, 1), 0, top)
    return jnp.take_along_axis(listing, (jnp.arange(top)[None, :] + offset_by) % top, axis=1)


def load_shares(number_of, total, reach, slope, full):
    portions = [(1 << 20) // math.isqrt(grade ** slope) + 1 for grade in range(1, number_of + 1)]
    largest = reach if full else min(reach, max(-(-total // number_of), total * portions[0] // sum(portions)))
    least = 1 if total - largest >= number_of - 1 else 0
    counts, spare = [largest] + [least] * (number_of - 1), total - largest - least * (number_of - 1)
    while spare > 0:
        free = [i for i in range(1, number_of) if counts[i] < largest] or [i for i in range(1, number_of) if counts[i] < reach]
        whole, remaining = sum([portions[i] for i in free]), spare
        for i in free:
            extra = min(reach - counts[i], max(1, remaining * portions[i] // whole), spare)
            counts[i] = counts[i] + extra
            spare = spare - extra
    return np.array(counts)


def scatter_about(own_key, extent, scale, limit, split=(), kind=jnp.bfloat16):
    entries = scale * jax.random.normal(own_key, extent, jnp.float32)
    if split:
        entries = entries * block_scale(own_key, extent, split, -0.22, 0.18)
    return jnp.clip(entries, -limit, limit).astype(kind)


def setup_inputs(seed: int = 0) -> dict:
    splits = jax.random.split(jax.random.key(seed), 8)
    tokens = scatter_about(splits[0], (TOKENS, D), 1.0, 6.0, ((0, 8),))
    norm_gain = jnp.clip(1.0 + 0.18 * jax.random.normal(splits[1], (D,), jnp.float32), 0.1, 1.9)
    route_ids_keys = jax.random.split(jax.random.fold_in(splits[2], 1), TOKENS // TOK_DEV)
    route_ids_turns = jax.random.permutation(jax.random.fold_in(splits[2], 3), TOKENS // TOK_DEV)
    route_ids = jax.vmap(lambda own, number: assign_block(jax.random.fold_in(splits[2], 2), own, number, TOK_DEV, EXPERTS, TOP_K, CAP, 2))(route_ids_keys, route_ids_turns).reshape((TOKENS, TOP_K))
    route_weights = jnp.clip(0.1 + 0.9 * jax.random.uniform(splits[3], (TOKENS, TOP_K), jnp.float32) ** block_scale(splits[3], (TOKENS, TOP_K), ((0, 8),), -0.2, 0.2), 0.1, 1.0)
    w_gate = scatter_about(splits[4], (EXPERTS, D, FF), (2.5 * D ** -0.5), 0.33007812, ((0, 8), (2, 4)))
    w_up = scatter_about(splits[5], (EXPERTS, D, FF), (2.5 * D ** -0.5), 0.33007812, ((0, 8), (2, 4)))
    w_down = scatter_about(splits[6], (EXPERTS, FF, D), (0.2 * FF ** -0.5), 0.026489258, ((0, 8), (2, 4)))
    return {"tokens": tokens, "norm_gain": norm_gain, "route_ids": route_ids, "route_weights": route_weights, "w_gate": w_gate, "w_up": w_up, "w_down": w_down}


swiglu_limit = 7.0
swiglu_alpha = 1.702
norm_eps = 1e-05

def clamped_units(gate_pre, up_pre):
    capped = jnp.minimum(gate_pre, swiglu_limit)
    linear = jnp.clip(up_pre, -swiglu_limit, swiglu_limit)
    return capped * jax.nn.sigmoid(swiglu_alpha * capped) * (linear + 1.0)

def slots_of(group_ids):
    matches = (group_ids[:, None] == jnp.arange(EXPERTS, dtype=jnp.int32)[None, :]).astype(jnp.int32)
    earlier = jnp.cumsum(matches, axis=0) - matches
    return lax.optimization_barrier(jnp.sum(earlier * matches, axis=1)).astype(jnp.int32)

def one_expert(args):
    row_block, gate_weight, up_weight, down_weight = args
    row_values = row_block.astype(jnp.float32)
    gate_pre = jnp.dot(row_values, gate_weight.astype(jnp.float32), preferred_element_type=jnp.float32)
    up_pre = jnp.dot(row_values, up_weight.astype(jnp.float32), preferred_element_type=jnp.float32)
    activation = clamped_units(gate_pre, up_pre).astype(jnp.bfloat16)
    result = jnp.dot(activation.astype(jnp.float32), down_weight.astype(jnp.float32), preferred_element_type=jnp.float32)
    return result.astype(jnp.bfloat16)

def reference(tokens, norm_gain, route_ids, route_weights, w_gate, w_up, w_down):
    values = tokens.astype(jnp.float32)
    row_mean = lax.optimization_barrier(jnp.mean(values, axis=1, keepdims=True))
    centred = values - row_mean
    row_var = lax.optimization_barrier(jnp.mean(centred * centred, axis=1, keepdims=True))
    normed = (centred * lax.rsqrt(row_var + norm_eps) * norm_gain).astype(jnp.bfloat16)
    group_ids = route_ids.reshape(N_EP, TOK_DEV * TOP_K).astype(jnp.int32)
    slot_index = lax.map(slots_of, group_ids)
    group_rank = jnp.arange(N_EP, dtype=jnp.int32)[:, None]
    position = (group_ids * (N_EP * CAP) + group_rank * CAP + slot_index).reshape(-1).astype(jnp.int32)
    source_rows = jnp.repeat(normed, TOP_K, axis=0)
    buffer = jnp.zeros((EXPERTS * N_EP * CAP, D), jnp.bfloat16).at[position].set(source_rows)
    results = lax.map(one_expert, (buffer.reshape(EXPERTS, N_EP * CAP, D), w_gate, w_up, w_down))
    picked = results.reshape(EXPERTS * N_EP * CAP, D)[position].reshape(TOKENS, TOP_K, D).astype(jnp.float32)
    return lax.optimization_barrier(jnp.sum(picked * route_weights[:, :, None], axis=1)).astype(jnp.bfloat16)
```

```python
import functools
import jax
import jax.numpy as jnp
from jax import lax
from jax.experimental import pallas as pl
from jax.experimental.pallas import tpu as pltpu
from jax.sharding import PartitionSpec as P

swiglu_limit = 7.0
swiglu_alpha = 1.702
norm_eps = 1e-05


def clamped_units(gate_pre, up_pre):
    capped = jnp.minimum(gate_pre, swiglu_limit)
    linear = jnp.clip(up_pre, -swiglu_limit, swiglu_limit)
    return capped * jax.nn.sigmoid(swiglu_alpha * capped) * (linear + 1.0)


def expert_work(outgoing, gate_weight, up_weight, down_weight):
    received = lax.all_to_all(outgoing, "ep", split_axis=1, concat_axis=1, tiled=True)
    local_count, sources, capacity, columns = received.shape
    row_count = sources * capacity
    row_block = received.reshape(local_count, row_count, columns)
    shard_piece = lax.all_gather(row_block, "tp", axis=2, tiled=True)
    gate_sum = jnp.einsum(
        "lrd,ldf->lrf", shard_piece, gate_weight, preferred_element_type=jnp.float32
    )
    up_sum = jnp.einsum("lrd,ldf->lrf", shard_piece, up_weight, preferred_element_type=jnp.float32)
    activation = clamped_units(gate_sum, up_sum).astype(jnp.bfloat16)
    out_cols = down_weight.shape[2]
    result = jnp.einsum(
        "lrf,lfd->lrd",
        lax.all_gather(activation, "tp", axis=2, tiled=True),
        down_weight,
        preferred_element_type=jnp.float32,
    )
    result = result.astype(jnp.bfloat16).reshape(local_count, sources, capacity, out_cols)
    return lax.all_to_all(result, "ep", split_axis=1, concat_axis=1, tiled=True)


def per_device(tokens, norm_gain, route_ids, route_weights, w_gate, w_up, w_down):
    local_count = w_gate.shape[0]
    sources = lax.axis_size("ep")
    tp_count = lax.axis_size("tp")
    width = tokens.shape[1]
    columns = width // tp_count
    experts = local_count * sources
    tok_rows, top_count = route_ids.shape
    capacity = 3 * tok_rows * top_count // (2 * experts)
    values = tokens.astype(jnp.float32)
    row_mean = jnp.mean(values, axis=1, keepdims=True)
    centred = values - row_mean
    row_var = jnp.mean(centred * centred, axis=1, keepdims=True)
    offset = lax.axis_index("tp") * columns
    own_cols = lax.dynamic_slice_in_dim(centred, offset, columns, 1)
    own_gain = lax.dynamic_slice_in_dim(norm_gain, offset, columns, 0)
    normed = (own_cols * lax.rsqrt(row_var + norm_eps) * own_gain).astype(jnp.bfloat16)
    flat_ids = route_ids.reshape(-1)
    matches = (flat_ids[:, None] == jnp.arange(experts, dtype=jnp.int32)[None, :]).astype(jnp.int32)
    earlier = jnp.cumsum(matches, axis=0) - matches
    slot_index = jnp.sum(earlier * matches, axis=1)
    position = (
        flat_ids % local_count * (sources * capacity)
        + flat_ids // local_count * capacity
        + slot_index
    )
    buffer_rows = local_count * sources * capacity
    placed = (
        position.reshape(tok_rows, top_count)[:, :, None]
        == jnp.arange(buffer_rows, dtype=jnp.int32)[None, None, :]
    )
    placement_matrix = jnp.any(placed, axis=1).astype(jnp.bfloat16)
    outgoing = jnp.einsum("tp,td->pd", placement_matrix, normed, preferred_element_type=jnp.float32)
    outgoing = outgoing.astype(jnp.bfloat16).reshape(local_count, sources, capacity, columns)
    returned = jnp.concatenate(
        [
            expert_work(
                outgoing[number : number + 1],
                w_gate[number : number + 1],
                w_up[number : number + 1],
                w_down[number : number + 1],
            )
            for number in range(local_count)
        ],
        axis=0,
    )
    flat_out = returned.reshape(buffer_rows, columns)
    picked = flat_out[position].reshape(tok_rows, top_count, columns).astype(jnp.float32)
    return jnp.sum(picked * route_weights[:, :, None], axis=1).astype(jnp.bfloat16)


CUT_EIGHTHS = 6
STAGES = (
    ("F", 1),
    ("L", 1, 0, 0),
    ("W", 1),
    ("L", 1, 0, 1),
    ("L", 1, 1, 0),
    ("S", 1, 0),
    ("L", 1, 1, 1),
    ("W", 0),
    ("F", 2),
    ("S", 1, 1),
    ("F", 3),
    ("W", 2),
    ("L", 2, 1, 0),
    ("L", 2, 1, 1),
    ("W", 3),
    ("S", 2, 1),
    ("L", 2, 0, 0),
    ("D", 2),
    ("L", 3, 1, 1),
    ("L", 3, 1, 0),
    ("F", 5),
    ("L", 3, 0, 0),
    ("S", 3, 1),
    ("R", 2),
    ("L", 2, 0, 1),
    ("D", 3),
    ("F", 7),
    ("D", 0),
    ("W", 5),
    ("L", 3, 0, 1),
    ("S", 3, 0),
    ("W", 7),
    ("F", 6),
    ("S", 2, 0),
    ("D", 5),
    ("F", 4),
    ("R", 5),
    ("D", 7),
    ("R", 7),
    ("W", 6),
    ("R", 3),
    ("W", 4),
    ("D", 6),
    ("R", 6),
    ("D", 4),
    ("D", 1),
    ("R", 4),
    ("R", 1),
)


def layer_kernel(
    capacity,
    tokens_hbm,
    gain_hbm,
    ids_hbm,
    mix_hbm,
    gate_hbm,
    up_hbm,
    down_hbm,
    out_ref,
    gate_w,
    up_w,
    down_w,
    tok_in,
    gain_in,
    ids_in,
    mix_in,
    toks,
    meta,
    earlier,
    rows,
    acts,
    weighted,
    combined,
    pair_out,
    pair_in,
    back_out,
    back_in,
    weight_sem,
    tok_sem,
    local_sem,
    meta_send,
    meta_recv,
    own_send,
    own_recv,
    line_send,
    line_recv,
    side_send,
    side_recv,
    mate_send,
    mate_recv,
    act_send,
    act_recv,
    pair_send,
    pair_recv,
    back_send,
    back_recv,
):
    sources = toks.shape[0]
    chips = sources // 2
    local_count = gate_w.shape[0]
    units = gate_w.shape[2]
    tok_rows = tok_in.shape[0]
    quarter = toks.shape[4]
    out_cols = down_w.shape[2]
    half_rows = tok_rows // 2
    cut = tok_rows * CUT_EIGHTHS // 8
    me = lax.axis_index("ep")
    tp = lax.axis_index("tp")
    z, core = me // 2, me % 2
    y, x = tp // 2, tp % 2
    tp_x = y * 2 + (1 - x)
    tp_y = (1 - y) * 2 + x
    side_tp = tp_x * (1 - core) + tp_y * core
    mate = z * 2 + (1 - core)
    own_half = (x + y) % 2
    parts = 2 if cut < tok_rows else 1

    def partner(k):
        chosen_chip = 0 * z
        for at in range(chips):
            sign = 1 if 2 * at < chips else -1
            order = sorted(range(chips), key=lambda c: (abs(c - at), sign * c))
            gap = (z - at) * (z - at)
            chosen_chip = chosen_chip + order[k] * (1 - (gap + chips * chips - 1) // (chips * chips))
        return chosen_chip

    def place(ep, column):
        return {"ep": ep, "tp": column}

    def remote(source, target, send, recv, where):
        return pltpu.make_async_remote_copy(
            src_ref=source,
            dst_ref=target,
            send_sem=send,
            recv_sem=recv,
            device_id=where,
            device_id_type=pl.DeviceIdType.MESH,
        )

    barrier = pltpu.get_barrier_semaphore()
    for d in range(1, sources):
        pl.semaphore_signal(
            barrier, inc=1, device_id=place((me + d) % sources, tp), device_id_type=pl.DeviceIdType.MESH
        )
    for column in (tp_x, tp_y):
        pl.semaphore_signal(
            barrier, inc=1, device_id=place(me, column), device_id_type=pl.DeviceIdType.MESH
        )

    piece_count = tok_sem.shape[0]
    piece_rows = tok_rows // piece_count
    tok_loads = [
        pltpu.make_async_copy(
            tokens_hbm.at[pl.ds(n * piece_rows, piece_rows)],
            tok_in.at[pl.ds(n * piece_rows, piece_rows)],
            tok_sem.at[n],
        )
        for n in range(piece_count)
    ]
    small = [
        pltpu.make_async_copy(gain_hbm, gain_in, local_sem.at[0]),
        pltpu.make_async_copy(ids_hbm, ids_in.at[me], local_sem.at[1]),
        pltpu.make_async_copy(mix_hbm, mix_in.at[me], local_sem.at[2]),
    ]
    loads = [
        pltpu.make_async_copy(hbm, vmem, weight_sem.at[n])
        for n, (hbm, vmem) in enumerate(((gate_hbm, gate_w), (up_hbm, up_w), (down_hbm, down_w)))
    ]
    for copy in small + tok_loads + loads:
        copy.start()

    before = lax.broadcasted_iota(jnp.int32, (tok_rows, tok_rows), 0)
    after = lax.broadcasted_iota(jnp.int32, (tok_rows, tok_rows), 1)
    earlier[...] = (before < after).astype(jnp.float32).astype(jnp.bfloat16)

    def make_meta(source):
        ids, mix = ids_in[source], mix_in[source]
        named, scales = [], []
        for n in range(local_count):
            match = ids == me * local_count + n
            named.append(jnp.sum(match.astype(jnp.float32), axis=0, keepdims=True))
            scales.append(jnp.sum(jnp.where(match, mix, 0.0), axis=0, keepdims=True))
        pad = [jnp.zeros((1, tok_rows), jnp.float32)] * (8 - local_count)
        names = jnp.concatenate(named + pad, axis=0)
        slot = jnp.dot(names.astype(jnp.bfloat16), earlier[...], preferred_element_type=jnp.float32)
        slot = jnp.where(names > 0.0, slot, -1.0)
        meta[source, 0] = slot
        meta[source, 1] = jnp.concatenate(scales + pad, axis=0)

    for copy in small:
        copy.wait()
    band = 32

    @pl.loop(0, piece_count)
    def _(p):
        pltpu.make_async_copy(
            tokens_hbm.at[pl.ds(0, piece_rows)], tok_in.at[pl.ds(0, piece_rows)], tok_sem.at[p]
        ).wait()
        for n in range(piece_rows // band):
            at = pl.ds(pl.multiple_of(p * piece_rows + n * band, band), band)
            values = tok_in[at, :].astype(jnp.float32)
            centred = values - jnp.mean(values, axis=1, keepdims=True)
            row_var = jnp.mean(centred * centred, axis=1, keepdims=True)
            normal = (centred * lax.rsqrt(row_var + norm_eps) * gain_in[...]).astype(jnp.bfloat16)
            for q in range(4):
                toks[me, q // 2, q % 2, at, :] = normal[:, q * quarter : (q + 1) * quarter]

    pending = []

    def go(copy):
        copy.start()
        pending.append(copy)
        return copy

    def always(condition, copy):
        pending.append((condition, copy))

    def line(chip, i, e, up):
        source = chip * 2 + i
        if e == 0:
            piece = toks.at[source, own_half, core]
        else:
            piece = toks.at[source, 1 - own_half, core, pl.ds(cut, tok_rows - cut)]
        return remote(
            piece,
            piece,
            line_send.at[up, chip, i, e],
            line_recv.at[chip, i, e],
            place((z + 2 * up - 1) * 2 + core, tp),
        )

    def side(chip, i):
        piece = toks.at[chip * 2 + i, own_half, core, pl.ds(0, cut)]
        return remote(
            piece, piece, side_send.at[chip, i], side_recv.at[chip, i], place(me, side_tp)
        )

    def to_mate(chip, i, m):
        source = chip * 2 + i
        piece = (
            toks.at[source, own_half, core],
            toks.at[source, 1 - own_half, core, pl.ds(cut, tok_rows - cut)] if parts > 1 else None,
            toks.at[source, 1 - own_half, core, pl.ds(0, cut)],
        )[m]
        return remote(
            piece, piece, mate_send.at[chip, i, m], mate_recv.at[chip, i, m], place(mate, tp)
        )

    mate_parts = (0, 1, 2) if parts > 1 else (0, 2)
    ends = ((1, z < chips - 1), (0, z > 0))

    def start_line(i):
        for e in range(parts):
            for up, there in ends:

                @pl.when(there)
                def _():
                    line(z, i, e, up).start()

    own_pieces = (
        toks.at[me, own_half, 1 - core],
        toks.at[me, 1 - own_half, 1 - core],
        toks.at[me, :, core],
    )
    own_copies = []
    metas = []
    acts_sent = {}

    def run_start():
        pl.semaphore_wait(barrier, sources + 1)
        for n, piece in enumerate(own_pieces):
            own_copies.append(
                go(remote(piece, piece, own_send.at[n], own_recv.at[n], place(mate, tp)))
            )

        @pl.when(core == 0)
        def _():
            start_line(0)

        send_act(0)
        for d in range(1, sources):
            for n, table in enumerate((ids_in, mix_in)):
                metas.append(
                    go(
                        remote(
                            table.at[me],
                            table.at[me],
                            meta_send.at[n, d],
                            meta_recv.at[n, d],
                            place((me + d) % sources, tp),
                        )
                    )
                )
        own_copies[0].wait_recv()
        own_copies[1].wait_recv()

        @pl.when(core == 1)
        def _():
            start_line(0)

        start_line(1)
        for up, there in ends:
            for i in range(2):
                for e in range(parts):
                    always(there, line(z, i, e, up))
        for copy in metas:
            copy.wait_recv()

        @pl.loop(1, sources)
        def _(d):
            make_meta((me + d) % sources)

    def run_line(distance, i, e):
        for up, chip in ((1, z - distance), (0, z + distance)):
            here = chip >= 0 if up else chip < chips
            ahead = z + 2 * up - 1
            onward = jnp.logical_and(here, ahead < chips if up else ahead >= 0)

            @pl.when(here)
            def _():
                line(chip, i, e, up).wait_recv()

                @pl.when(ahead < chips if up else ahead >= 0)
                def _():
                    line(chip, i, e, up).start()

                if e == 0:
                    side(chip, i).start()
                to_mate(chip, i, e).start()

            always(onward, line(chip, i, e, up))
            if e == 0:
                always(here, side(chip, i))
            always(here, to_mate(chip, i, e))

    def run_side(k, i):
        chip = partner(k)
        side(chip, i).wait_recv()
        go(to_mate(chip, i, 2))

    def chosen(source):
        slots, scales = meta[source, 0], meta[source, 1]
        at = lax.broadcasted_iota(jnp.int32, (capacity, tok_rows), 0).astype(jnp.float32)
        hits = [at == slots[n : n + 1, :] for n in range(local_count)]
        ones = jnp.concatenate([h.astype(jnp.float32) for h in hits], axis=0)
        scale = jnp.concatenate(
            [
                jnp.sum(jnp.where(hits[n], scales[n : n + 1, :], 0.0), axis=1, keepdims=True)
                for n in range(local_count)
            ],
            axis=0,
        )
        return ones.astype(jnp.bfloat16), scale

    def source_of(s):
        if s == 0:
            return me
        if s == 1:
            return mate
        return partner(s // 2) * 2 + s % 2

    def compute_act(s):
        source = source_of(s)
        ones, _ = chosen(source)
        for q in range(4):
            got = jnp.dot(ones, toks[source, q // 2, q % 2], preferred_element_type=jnp.float32)
            got = got.astype(jnp.bfloat16)
            for n in range(local_count):
                rows[n, :, q * quarter : (q + 1) * quarter] = got[n * capacity : (n + 1) * capacity]

        @pl.loop(0, local_count)
        def _(n):
            block = rows[n]
            half = units // 2
            for part in range(2):
                cols = slice(part * half, (part + 1) * half)
                gate = jnp.dot(block, gate_w[n, :, cols], preferred_element_type=jnp.float32)
                up = jnp.dot(block, up_w[n, :, cols], preferred_element_type=jnp.float32)
                acts[s, tp, n, :, cols] = clamped_units(gate, up).astype(jnp.bfloat16)

    def send_act(s):
        piece = acts.at[s, tp]
        acts_sent[s] = [
            go(remote(piece, piece, act_send.at[s, n], act_recv.at[s, n], place(me, column)))
            for n, column in enumerate((tp_x, tp_y))
        ]

    def run_first(s):
        if s == 1:
            own_copies[2].wait_recv()
        elif s > 1:
            chip = partner(s // 2)
            for m in mate_parts:
                to_mate(chip, s % 2, m).wait_recv()
        compute_act(s)
        send_act(s)

    def run_forward(s):
        mid = local_count // 2
        for n, (origin, column, at, size) in enumerate(
            ((tp_x, tp_y, 0, mid), (tp_y, tp_x, mid, local_count - mid))
        ):
            acts_sent[s][n].wait_recv()
            piece = acts.at[s, origin, pl.ds(at, size)]
            acts_sent[s].append(
                go(
                    remote(
                        piece, piece, act_send.at[s, 2 + n], act_recv.at[s, 2 + n], place(me, column)
                    )
                )
            )

    pairs = {}

    def run_second(s):
        acts_sent[s][2].wait_recv()
        acts_sent[s][3].wait_recv()

        @pl.loop(0, local_count)
        def _(n):
            total = jnp.zeros((capacity, out_cols), jnp.float32)
            for t in range(acts.shape[1]):
                total = total + jnp.dot(
                    acts[s, t, n],
                    down_w[n, t * units : (t + 1) * units, :],
                    preferred_element_type=jnp.float32,
                )
            weighted[n] = total

        ones, scale = chosen(source_of(s))
        value = jnp.concatenate([weighted[n] for n in range(local_count)], axis=0)
        value = (value * scale).astype(jnp.bfloat16)
        result = lax.dot_general(
            ones, value, (((0,), (0,)), ((), ())), preferred_element_type=jnp.float32
        )
        for h in range(2):
            combined[s, h] = result[h * half_rows : (h + 1) * half_rows]
        if s == 1:
            for h in range(2):
                pair_out[0, h] = combined[1, h].astype(jnp.bfloat16)
            piece, target = pair_out.at[0], pair_in.at[0]
        elif s > 1:
            pair_out[s // 2, s % 2] = combined[s, 1 - core].astype(jnp.bfloat16)
            piece, target = pair_out.at[s // 2, s % 2], pair_in.at[s // 2, s % 2]
        if s > 0:
            pairs[s] = go(remote(piece, target, pair_send.at[s], pair_recv.at[s], place(mate, tp)))

    def run_back(s):
        pairs[s].wait_recv()
        if s > 1:
            k, i = s // 2, s % 2
            both = combined[s, core] + pair_in[k, i].astype(jnp.float32)
            back_out[k, i] = both.astype(jnp.bfloat16)
            go(
                remote(
                    back_out.at[k, i],
                    back_in.at[z, core],
                    back_send.at[k, i],
                    back_recv.at[z, core],
                    place(partner(k) * 2 + i, tp),
                )
            )

    make_meta(me)
    loads[0].wait()
    loads[1].wait()
    compute_act(0)
    run_start()
    loads[2].wait()
    runs = {
        "L": run_line,
        "S": run_side,
        "F": run_first,
        "W": run_forward,
        "D": run_second,
        "R": run_back,
    }
    for kind, *rest in STAGES:
        runs[kind](*rest)
    for h in range(2):
        result = combined[0, h] + pair_in[0, h].astype(jnp.float32)
        for d in range(1, chips):
            chip = (z + d) % chips
            remote(
                back_out.at[0, 0], back_in.at[chip, h], back_send.at[0, h], back_recv.at[chip, h], place(mate, tp)
            ).wait_recv()
            result = result + back_in[chip, h].astype(jnp.float32)
        out_ref[h * half_rows : (h + 1) * half_rows, :] = result.astype(out_ref.dtype)
    for entry in pending:
        if isinstance(entry, tuple):

            @pl.when(entry[0])
            def _():
                entry[1].wait_send()
        else:
            entry.wait_send()


def fused_per_device(tokens, norm_gain, route_ids, route_weights, w_gate, w_up, w_down):
    local_count, width, units = w_gate.shape
    out_cols = w_down.shape[2]
    sources = lax.axis_size("ep")
    tp_count = lax.axis_size("tp")
    experts = local_count * sources
    tok_rows, top_count = route_ids.shape
    capacity = 3 * tok_rows * top_count // (2 * experts)
    chips = sources // 2
    quarter = width // 4
    half_rows = tok_rows // 2
    dma = pltpu.SemaphoreType.DMA
    bf16 = jnp.bfloat16
    vmem = pl.BlockSpec(memory_space=pltpu.VMEM)
    hbm = pl.BlockSpec(memory_space=pltpu.HBM)
    return pl.pallas_call(
        functools.partial(layer_kernel, capacity),
        out_shape=jax.ShapeDtypeStruct((tok_rows, out_cols), bf16),
        in_specs=[hbm] * 7,
        out_specs=vmem,
        scratch_shapes=[
            pltpu.VMEM(w_gate.shape, bf16),
            pltpu.VMEM(w_up.shape, bf16),
            pltpu.VMEM(w_down.shape, bf16),
            pltpu.VMEM(tokens.shape, bf16),
            pltpu.VMEM((1, width), jnp.float32),
            pltpu.VMEM((sources, top_count, tok_rows), jnp.int32),
            pltpu.VMEM((sources, top_count, tok_rows), jnp.float32),
            pltpu.VMEM((sources, 2, 2, tok_rows, quarter), bf16),
            pltpu.VMEM((sources, 2, 8, tok_rows), jnp.float32),
            pltpu.VMEM((tok_rows, tok_rows), bf16),
            pltpu.VMEM((local_count, capacity, width), bf16),
            pltpu.VMEM((sources, tp_count, local_count, capacity, units), bf16),
            pltpu.VMEM((local_count, capacity, out_cols), jnp.float32),
            pltpu.VMEM((sources, 2, half_rows, out_cols), jnp.float32),
            pltpu.VMEM((chips, 2, half_rows, out_cols), bf16),
            pltpu.VMEM((chips, 2, half_rows, out_cols), bf16),
            pltpu.VMEM((chips, 2, half_rows, out_cols), bf16),
            pltpu.VMEM((chips, 2, half_rows, out_cols), bf16),
            dma((3,)),
            dma((4,)),
            dma((3,)),
            dma((2, sources)),
            dma((2, sources)),
            dma((3,)),
            dma((3,)),
            dma((2, chips, 2, 2)),
            dma((chips, 2, 2)),
            dma((chips, 2)),
            dma((chips, 2)),
            dma((chips, 2, 3)),
            dma((chips, 2, 3)),
            dma((sources, 4)),
            dma((sources, 4)),
            dma((sources,)),
            dma((sources,)),
            dma((chips, 2)),
            dma((chips, 2)),
        ],
        compiler_params=pltpu.CompilerParams(
            collective_id=0, has_side_effects=True, vmem_limit_bytes=60 * 1024 * 1024
        ),
    )(tokens, norm_gain.reshape(1, width), route_ids.T, route_weights.T, w_gate, w_up, w_down)


def pick_plan(mesh):
    sources, tp_count = mesh.shape["ep"], mesh.shape["tp"]

    def body(tokens, norm_gain, route_ids, route_weights, w_gate, w_up, w_down):
        tok_rows, top_count = route_ids.shape
        experts = w_gate.shape[0] * sources
        capacity = 3 * tok_rows * top_count // (2 * experts)
        gathered = 2 * tokens.size * sources + 6 * w_gate.size
        fused = (
            tp_count == 4
            and sources == 8
            and capacity % 16 == 0
            and w_gate.shape[0] in (2, 4, 6, 8)
            and tok_rows % 128 == 0
            and tokens.shape[1] % 512 == 0
            and gathered < 32 * 1024 * 1024
        )
        run = fused_per_device if fused else per_device
        return run(tokens, norm_gain, route_ids, route_weights, w_gate, w_up, w_down)

    return body


def solution(mesh):
    return jax.shard_map(
        pick_plan(mesh),
        mesh=mesh,
        in_specs=(
            P("ep", None),
            P(),
            P("ep", None),
            P("ep", None),
            P("ep", None, "tp"),
            P("ep", None, "tp"),
            P("ep", None, "tp"),
        ),
        out_specs=P("ep", "tp"),
        check_vma=False,
    )
```

```python
import functools
import jax
import jax.numpy as jnp
from jax import lax
from jax.experimental import pallas as pl
from jax.experimental.pallas import tpu as pltpu
from jax.sharding import PartitionSpec as P

swiglu_limit = 7.0
swiglu_alpha = 1.702
norm_eps = 1e-05


def clamped_units(gate_pre, up_pre):
    capped = jnp.minimum(gate_pre, swiglu_limit)
    linear = jnp.clip(up_pre, -swiglu_limit, swiglu_limit)
    return capped * jax.nn.sigmoid(swiglu_alpha * capped) * (linear + 1.0)


def expert_work(outgoing, gate_weight, up_weight, down_weight):
    received = lax.all_to_all(outgoing, "ep", split_axis=1, concat_axis=1, tiled=True)
    local_count, sources, capacity, columns = received.shape
    row_count = sources * capacity
    row_block = received.reshape(local_count, row_count, columns)
    shard_piece = lax.all_gather(row_block, "tp", axis=2, tiled=True)
    gate_sum = jnp.einsum(
        "lrd,ldf->lrf", shard_piece, gate_weight, preferred_element_type=jnp.float32
    )
    up_sum = jnp.einsum("lrd,ldf->lrf", shard_piece, up_weight, preferred_element_type=jnp.float32)
    activation = clamped_units(gate_sum, up_sum).astype(jnp.bfloat16)
    out_cols = down_weight.shape[2]
    result = jnp.einsum(
        "lrf,lfd->lrd",
        lax.all_gather(activation, "tp", axis=2, tiled=True),
        down_weight,
        preferred_element_type=jnp.float32,
    )
    result = result.astype(jnp.bfloat16).reshape(local_count, sources, capacity, out_cols)
    return lax.all_to_all(result, "ep", split_axis=1, concat_axis=1, tiled=True)


def per_device(tokens, norm_gain, route_ids, route_weights, w_gate, w_up, w_down):
    local_count = w_gate.shape[0]
    sources = lax.axis_size("ep")
    tp_count = lax.axis_size("tp")
    width = tokens.shape[1]
    columns = width // tp_count
    experts = local_count * sources
    tok_rows, top_count = route_ids.shape
    capacity = 3 * tok_rows * top_count // (2 * experts)
    values = tokens.astype(jnp.float32)
    row_mean = jnp.mean(values, axis=1, keepdims=True)
    centred = values - row_mean
    row_var = jnp.mean(centred * centred, axis=1, keepdims=True)
    offset = lax.axis_index("tp") * columns
    own_cols = lax.dynamic_slice_in_dim(centred, offset, columns, 1)
    own_gain = lax.dynamic_slice_in_dim(norm_gain, offset, columns, 0)
    normed = (own_cols * lax.rsqrt(row_var + norm_eps) * own_gain).astype(jnp.bfloat16)
    flat_ids = route_ids.reshape(-1)
    matches = (flat_ids[:, None] == jnp.arange(experts, dtype=jnp.int32)[None, :]).astype(jnp.int32)
    earlier = jnp.cumsum(matches, axis=0) - matches
    slot_index = jnp.sum(earlier * matches, axis=1)
    position = (
        flat_ids % local_count * (sources * capacity)
        + flat_ids // local_count * capacity
        + slot_index
    )
    buffer_rows = local_count * sources * capacity
    placed = (
        position.reshape(tok_rows, top_count)[:, :, None]
        == jnp.arange(buffer_rows, dtype=jnp.int32)[None, None, :]
    )
    placement_matrix = jnp.any(placed, axis=1).astype(jnp.bfloat16)
    outgoing = jnp.einsum("tp,td->pd", placement_matrix, normed, preferred_element_type=jnp.float32)
    outgoing = outgoing.astype(jnp.bfloat16).reshape(local_count, sources, capacity, columns)
    returned = jnp.concatenate(
        [
            expert_work(
                outgoing[number : number + 1],
                w_gate[number : number + 1],
                w_up[number : number + 1],
                w_down[number : number + 1],
            )
            for number in range(local_count)
        ],
        axis=0,
    )
    flat_out = returned.reshape(buffer_rows, columns)
    picked = flat_out[position].reshape(tok_rows, top_count, columns).astype(jnp.float32)
    return jnp.sum(picked * route_weights[:, :, None], axis=1).astype(jnp.bfloat16)


CUT_EIGHTHS = 6
STAGES = (
    ("L", 1, 0, 0),
    ("F", 1),
    ("L", 1, 0, 1),
    ("S", 1, 0),
    ("W", 0),
    ("F", 2),
    ("L", 1, 1, 1),
    ("L", 1, 1, 0),
    ("L", 2, 0, 0),
    ("W", 2),
    ("L", 2, 1, 1),
    ("L", 2, 0, 1),
    ("S", 2, 0),
    ("L", 2, 1, 0),
    ("F", 4),
    ("S", 2, 1),
    ("S", 1, 1),
    ("L", 3, 0, 0),
    ("F", 5),
    ("W", 4),
    ("F", 3),
    ("D", 0),
    ("L", 3, 0, 1),
    ("L", 3, 1, 0),
    ("W", 5),
    ("S", 3, 0),
    ("L", 3, 1, 1),
    ("F", 6),
    ("D", 4),
    ("D", 2),
    ("S", 3, 1),
    ("R", 2),
    ("R", 4),
    ("W", 3),
    ("D", 5),
    ("W", 6),
    ("F", 7),
    ("R", 5),
    ("D", 3),
    ("D", 6),
    ("R", 3),
    ("W", 7),
    ("W", 1),
    ("R", 6),
    ("D", 7),
    ("R", 7),
    ("D", 1),
    ("R", 1),
)


def layer_kernel(
    capacity,
    tokens_hbm,
    gain_hbm,
    ids_hbm,
    mix_hbm,
    gate_hbm,
    up_hbm,
    down_hbm,
    out_ref,
    gate_w,
    up_w,
    down_w,
    tok_in,
    gain_in,
    ids_in,
    mix_in,
    toks,
    meta,
    earlier,
    rows,
    acts,
    weighted,
    combined,
    pair_out,
    pair_in,
    back_out,
    back_in,
    weight_sem,
    tok_sem,
    local_sem,
    meta_send,
    meta_recv,
    own_send,
    own_recv,
    line_send,
    line_recv,
    side_send,
    side_recv,
    mate_send,
    mate_recv,
    act_send,
    act_recv,
    pair_send,
    pair_recv,
    back_send,
    back_recv,
):
    sources = toks.shape[0]
    chips = sources // 2
    local_count = gate_w.shape[0]
    units = gate_w.shape[2]
    tok_rows = tok_in.shape[0]
    quarter = toks.shape[4]
    out_cols = down_w.shape[2]
    half_rows = tok_rows // 2
    cut = tok_rows * CUT_EIGHTHS // 8
    me = lax.axis_index("ep")
    tp = lax.axis_index("tp")
    z, core = me // 2, me % 2
    y, x = tp // 2, tp % 2
    tp_x = y * 2 + (1 - x)
    tp_y = (1 - y) * 2 + x
    side_tp = tp_x * (1 - core) + tp_y * core
    mate = z * 2 + (1 - core)
    own_half = (x + y) % 2
    parts = 2 if cut < tok_rows else 1

    def partner(k):
        chosen_chip = 0 * z
        for at in range(chips):
            sign = 1 if 2 * at < chips else -1
            order = sorted(range(chips), key=lambda c: (abs(c - at), sign * c))
            gap = (z - at) * (z - at)
            chosen_chip = chosen_chip + order[k] * (1 - (gap + chips * chips - 1) // (chips * chips))
        return chosen_chip

    def place(ep, column):
        return {"ep": ep, "tp": column}

    def remote(source, target, send, recv, where):
        return pltpu.make_async_remote_copy(
            src_ref=source,
            dst_ref=target,
            send_sem=send,
            recv_sem=recv,
            device_id=where,
            device_id_type=pl.DeviceIdType.MESH,
        )

    barrier = pltpu.get_barrier_semaphore()
    for d in range(1, sources):
        pl.semaphore_signal(
            barrier, inc=1, device_id=place((me + d) % sources, tp), device_id_type=pl.DeviceIdType.MESH
        )
    for column in (tp_x, tp_y):
        pl.semaphore_signal(
            barrier, inc=1, device_id=place(me, column), device_id_type=pl.DeviceIdType.MESH
        )

    piece_count = tok_sem.shape[0]
    piece_rows = tok_rows // piece_count
    tok_loads = [
        pltpu.make_async_copy(
            tokens_hbm.at[pl.ds(n * piece_rows, piece_rows)],
            tok_in.at[pl.ds(n * piece_rows, piece_rows)],
            tok_sem.at[n],
        )
        for n in range(piece_count)
    ]
    small = [
        pltpu.make_async_copy(gain_hbm, gain_in, local_sem.at[0]),
        pltpu.make_async_copy(ids_hbm, ids_in.at[me], local_sem.at[1]),
        pltpu.make_async_copy(mix_hbm, mix_in.at[me], local_sem.at[2]),
    ]
    loads = [
        pltpu.make_async_copy(hbm, vmem, weight_sem.at[n])
        for n, (hbm, vmem) in enumerate(((gate_hbm, gate_w), (up_hbm, up_w), (down_hbm, down_w)))
    ]
    for copy in small + tok_loads:
        copy.start()

    before = lax.broadcasted_iota(jnp.int32, (tok_rows, tok_rows), 0)
    after = lax.broadcasted_iota(jnp.int32, (tok_rows, tok_rows), 1)
    earlier[...] = (before < after).astype(jnp.float32).astype(jnp.bfloat16)

    def make_meta(source):
        ids, mix = ids_in[source], mix_in[source]
        named, scales = [], []
        for n in range(local_count):
            match = ids == me * local_count + n
            named.append(jnp.sum(match.astype(jnp.float32), axis=0, keepdims=True))
            scales.append(jnp.sum(jnp.where(match, mix, 0.0), axis=0, keepdims=True))
        pad = [jnp.zeros((1, tok_rows), jnp.float32)] * (8 - local_count)
        names = jnp.concatenate(named + pad, axis=0)
        slot = jnp.dot(names.astype(jnp.bfloat16), earlier[...], preferred_element_type=jnp.float32)
        slot = jnp.where(names > 0.0, slot, -1.0)
        meta[source, 0] = slot
        meta[source, 1] = jnp.concatenate(scales + pad, axis=0)

    for copy in small + tok_loads:
        copy.wait()
    for copy in loads:
        copy.start()
    band = 32

    @pl.loop(0, piece_count)
    def _(p):
        for n in range(piece_rows // band):
            at = pl.ds(pl.multiple_of(p * piece_rows + n * band, band), band)
            values = tok_in[at, :].astype(jnp.float32)
            centred = values - jnp.mean(values, axis=1, keepdims=True)
            row_var = jnp.mean(centred * centred, axis=1, keepdims=True)
            normal = (centred * lax.rsqrt(row_var + norm_eps) * gain_in[...]).astype(jnp.bfloat16)
            for q in range(4):
                toks[me, q // 2, q % 2, at, :] = normal[:, q * quarter : (q + 1) * quarter]

    pending = []

    def go(copy):
        copy.start()
        pending.append(copy)
        return copy

    def always(condition, copy):
        pending.append((condition, copy))

    def line(chip, i, e, up):
        source = chip * 2 + i
        if e == 0:
            piece = toks.at[source, own_half, core]
        else:
            piece = toks.at[source, 1 - own_half, core, pl.ds(cut, tok_rows - cut)]
        return remote(
            piece,
            piece,
            line_send.at[up, chip, i, e],
            line_recv.at[chip, i, e],
            place((z + 2 * up - 1) * 2 + core, tp),
        )

    def side(chip, i):
        piece = toks.at[chip * 2 + i, own_half, core, pl.ds(0, cut)]
        return remote(
            piece, piece, side_send.at[chip, i], side_recv.at[chip, i], place(me, side_tp)
        )

    def to_mate(chip, i, m):
        source = chip * 2 + i
        piece = (
            toks.at[source, own_half, core],
            toks.at[source, 1 - own_half, core, pl.ds(cut, tok_rows - cut)] if parts > 1 else None,
            toks.at[source, 1 - own_half, core, pl.ds(0, cut)],
        )[m]
        return remote(
            piece, piece, mate_send.at[chip, i, m], mate_recv.at[chip, i, m], place(mate, tp)
        )

    mate_parts = (0, 1, 2) if parts > 1 else (0, 2)
    ends = ((1, z < chips - 1), (0, z > 0))

    def start_line(i):
        for e in range(parts):
            for up, there in ends:

                @pl.when(there)
                def _():
                    line(z, i, e, up).start()

    own_pieces = (
        toks.at[me, own_half, 1 - core],
        toks.at[me, 1 - own_half, 1 - core],
        toks.at[me, :, core],
    )
    own_copies = []
    metas = []
    acts_sent = {}

    def run_start():
        pl.semaphore_wait(barrier, sources + 1)
        for d in range(1, sources):
            for n, table in enumerate((ids_in, mix_in)):
                metas.append(
                    go(
                        remote(
                            table.at[me],
                            table.at[me],
                            meta_send.at[n, d],
                            meta_recv.at[n, d],
                            place((me + d) % sources, tp),
                        )
                    )
                )
        for n, piece in enumerate(own_pieces):
            own_copies.append(
                go(remote(piece, piece, own_send.at[n], own_recv.at[n], place(mate, tp)))
            )

        @pl.when(core == 0)
        def _():
            start_line(0)

        own_copies[0].wait_recv()
        own_copies[1].wait_recv()

        @pl.when(core == 1)
        def _():
            start_line(0)

        start_line(1)
        for up, there in ends:
            for i in range(2):
                for e in range(parts):
                    always(there, line(z, i, e, up))
    def run_line(distance, i, e):
        for up, chip in ((1, z - distance), (0, z + distance)):
            here = chip >= 0 if up else chip < chips
            ahead = z + 2 * up - 1
            onward = jnp.logical_and(here, ahead < chips if up else ahead >= 0)

            @pl.when(here)
            def _():
                line(chip, i, e, up).wait_recv()

                @pl.when(ahead < chips if up else ahead >= 0)
                def _():
                    line(chip, i, e, up).start()

                if e == 0:
                    side(chip, i).start()
                to_mate(chip, i, e).start()

            always(onward, line(chip, i, e, up))
            if e == 0:
                always(here, side(chip, i))
            always(here, to_mate(chip, i, e))

    def run_side(k, i):
        chip = partner(k)
        side(chip, i).wait_recv()
        go(to_mate(chip, i, 2))

    def chosen(source):
        slots, scales = meta[source, 0], meta[source, 1]
        at = lax.broadcasted_iota(jnp.int32, (capacity, tok_rows), 0).astype(jnp.float32)
        hits = [at == slots[n : n + 1, :] for n in range(local_count)]
        ones = jnp.concatenate([h.astype(jnp.float32) for h in hits], axis=0)
        scale = jnp.concatenate(
            [
                jnp.sum(jnp.where(hits[n], scales[n : n + 1, :], 0.0), axis=1, keepdims=True)
                for n in range(local_count)
            ],
            axis=0,
        )
        return ones.astype(jnp.bfloat16), scale

    def source_of(s):
        if s == 0:
            return me
        if s == 1:
            return mate
        return partner(s // 2) * 2 + s % 2

    def compute_act(s):
        source = source_of(s)
        ones, _ = chosen(source)
        for q in range(4):
            got = jnp.dot(ones, toks[source, q // 2, q % 2], preferred_element_type=jnp.float32)
            got = got.astype(jnp.bfloat16)
            for n in range(local_count):
                rows[n, :, q * quarter : (q + 1) * quarter] = got[n * capacity : (n + 1) * capacity]

        @pl.loop(0, local_count)
        def _(n):
            block = rows[n]
            half = units // 2
            for part in range(2):
                cols = slice(part * half, (part + 1) * half)
                gate = jnp.dot(block, gate_w[n, :, cols], preferred_element_type=jnp.float32)
                up = jnp.dot(block, up_w[n, :, cols], preferred_element_type=jnp.float32)
                acts[s, tp, n, :, cols] = clamped_units(gate, up).astype(jnp.bfloat16)

    def send_act(s):
        piece = acts.at[s, tp]
        acts_sent[s] = [
            go(remote(piece, piece, act_send.at[s, n], act_recv.at[s, n], place(me, column)))
            for n, column in enumerate((tp_x, tp_y))
        ]

    def run_first(s):
        while metas:
            metas.pop().wait_recv()
        make_meta(source_of(s))
        if s == 1:
            own_copies[2].wait_recv()
        elif s > 1:
            chip = partner(s // 2)
            for m in mate_parts:
                to_mate(chip, s % 2, m).wait_recv()
        compute_act(s)
        send_act(s)

    def run_forward(s):
        mid = local_count // 2
        for n, (origin, column, at, size) in enumerate(
            ((tp_x, tp_y, 0, mid), (tp_y, tp_x, mid, local_count - mid))
        ):
            acts_sent[s][n].wait_recv()
            piece = acts.at[s, origin, pl.ds(at, size)]
            acts_sent[s].append(
                go(
                    remote(
                        piece, piece, act_send.at[s, 2 + n], act_recv.at[s, 2 + n], place(me, column)
                    )
                )
            )

    pairs = {}

    def run_second(s):
        acts_sent[s][2].wait_recv()
        acts_sent[s][3].wait_recv()

        @pl.loop(0, local_count)
        def _(n):
            total = jnp.zeros((capacity, out_cols), jnp.float32)
            for t in range(acts.shape[1]):
                total = total + jnp.dot(
                    acts[s, t, n],
                    down_w[n, t * units : (t + 1) * units, :],
                    preferred_element_type=jnp.float32,
                )
            weighted[n] = total

        ones, scale = chosen(source_of(s))
        value = jnp.concatenate([weighted[n] for n in range(local_count)], axis=0)
        value = (value * scale).astype(jnp.bfloat16)
        result = lax.dot_general(
            ones, value, (((0,), (0,)), ((), ())), preferred_element_type=jnp.float32
        )
        for h in range(2):
            combined[s, h] = result[h * half_rows : (h + 1) * half_rows]
        if s == 1:
            for h in range(2):
                pair_out[0, h] = combined[1, h].astype(jnp.bfloat16)
            piece, target = pair_out.at[0], pair_in.at[0]
        elif s > 1:
            pair_out[s // 2, s % 2] = combined[s, 1 - core].astype(jnp.bfloat16)
            piece, target = pair_out.at[s // 2, s % 2], pair_in.at[s // 2, s % 2]
        if s > 0:
            pairs[s] = go(remote(piece, target, pair_send.at[s], pair_recv.at[s], place(mate, tp)))

    def run_back(s):
        pairs[s].wait_recv()
        if s > 1:
            k, i = s // 2, s % 2
            both = combined[s, core] + pair_in[k, i].astype(jnp.float32)
            back_out[k, i] = both.astype(jnp.bfloat16)
            go(
                remote(
                    back_out.at[k, i],
                    back_in.at[z, core],
                    back_send.at[k, i],
                    back_recv.at[z, core],
                    place(partner(k) * 2 + i, tp),
                )
            )

    run_start()
    make_meta(me)
    loads[0].wait()
    loads[1].wait()
    compute_act(0)
    send_act(0)
    loads[2].wait()
    runs = {
        "L": run_line,
        "S": run_side,
        "F": run_first,
        "W": run_forward,
        "D": run_second,
        "R": run_back,
    }
    for kind, *rest in STAGES:
        runs[kind](*rest)
    for h in range(2):
        result = combined[0, h] + pair_in[0, h].astype(jnp.float32)
        for d in range(1, chips):
            chip = (z + d) % chips
            remote(
                back_out.at[0, 0], back_in.at[chip, h], back_send.at[0, h], back_recv.at[chip, h], place(mate, tp)
            ).wait_recv()
            result = result + back_in[chip, h].astype(jnp.float32)
        out_ref[h * half_rows : (h + 1) * half_rows, :] = result.astype(out_ref.dtype)
    for entry in pending:
        if isinstance(entry, tuple):

            @pl.when(entry[0])
            def _():
                entry[1].wait_send()
        else:
            entry.wait_send()


def fused_per_device(tokens, norm_gain, route_ids, route_weights, w_gate, w_up, w_down):
    local_count, width, units = w_gate.shape
    out_cols = w_down.shape[2]
    sources = lax.axis_size("ep")
    tp_count = lax.axis_size("tp")
    experts = local_count * sources
    tok_rows, top_count = route_ids.shape
    capacity = 3 * tok_rows * top_count // (2 * experts)
    chips = sources // 2
    quarter = width // 4
    half_rows = tok_rows // 2
    dma = pltpu.SemaphoreType.DMA
    bf16 = jnp.bfloat16
    vmem = pl.BlockSpec(memory_space=pltpu.VMEM)
    hbm = pl.BlockSpec(memory_space=pltpu.HBM)
    return pl.pallas_call(
        functools.partial(layer_kernel, capacity),
        out_shape=jax.ShapeDtypeStruct((tok_rows, out_cols), bf16),
        in_specs=[hbm] * 7,
        out_specs=vmem,
        scratch_shapes=[
            pltpu.VMEM(w_gate.shape, bf16),
            pltpu.VMEM(w_up.shape, bf16),
            pltpu.VMEM(w_down.shape, bf16),
            pltpu.VMEM(tokens.shape, bf16),
            pltpu.VMEM((1, width), jnp.float32),
            pltpu.VMEM((sources, top_count, tok_rows), jnp.int32),
            pltpu.VMEM((sources, top_count, tok_rows), jnp.float32),
            pltpu.VMEM((sources, 2, 2, tok_rows, quarter), bf16),
            pltpu.VMEM((sources, 2, 8, tok_rows), jnp.float32),
            pltpu.VMEM((tok_rows, tok_rows), bf16),
            pltpu.VMEM((local_count, capacity, width), bf16),
            pltpu.VMEM((sources, tp_count, local_count, capacity, units), bf16),
            pltpu.VMEM((local_count, capacity, out_cols), jnp.float32),
            pltpu.VMEM((sources, 2, half_rows, out_cols), jnp.float32),
            pltpu.VMEM((chips, 2, half_rows, out_cols), bf16),
            pltpu.VMEM((chips, 2, half_rows, out_cols), bf16),
            pltpu.VMEM((chips, 2, half_rows, out_cols), bf16),
            pltpu.VMEM((chips, 2, half_rows, out_cols), bf16),
            dma((3,)),
            dma((4,)),
            dma((3,)),
            dma((2, sources)),
            dma((2, sources)),
            dma((3,)),
            dma((3,)),
            dma((2, chips, 2, 2)),
            dma((chips, 2, 2)),
            dma((chips, 2)),
            dma((chips, 2)),
            dma((chips, 2, 3)),
            dma((chips, 2, 3)),
            dma((sources, 4)),
            dma((sources, 4)),
            dma((sources,)),
            dma((sources,)),
            dma((chips, 2)),
            dma((chips, 2)),
        ],
        compiler_params=pltpu.CompilerParams(
            collective_id=0, has_side_effects=True, vmem_limit_bytes=60 * 1024 * 1024
        ),
    )(tokens, norm_gain.reshape(1, width), route_ids.T, route_weights.T, w_gate, w_up, w_down)


def pick_plan(mesh):
    sources, tp_count = mesh.shape["ep"], mesh.shape["tp"]

    def body(tokens, norm_gain, route_ids, route_weights, w_gate, w_up, w_down):
        tok_rows, top_count = route_ids.shape
        experts = w_gate.shape[0] * sources
        capacity = 3 * tok_rows * top_count // (2 * experts)
        gathered = 2 * tokens.size * sources + 6 * w_gate.size
        fused = (
            tp_count == 4
            and sources == 8
            and capacity % 16 == 0
            and w_gate.shape[0] in (2, 4, 6, 8)
            and tok_rows % 128 == 0
            and tokens.shape[1] % 512 == 0
            and gathered < 32 * 1024 * 1024
        )
        run = fused_per_device if fused else per_device
        return run(tokens, norm_gain, route_ids, route_weights, w_gate, w_up, w_down)

    return body


def solution(mesh):
    return jax.shard_map(
        pick_plan(mesh),
        mesh=mesh,
        in_specs=(
            P("ep", None),
            P(),
            P("ep", None),
            P("ep", None),
            P("ep", None, "tp"),
            P("ep", None, "tp"),
            P("ep", None, "tp"),
        ),
        out_specs=P("ep", "tp"),
        check_vma=False,
    )
```

```python
import functools
import jax
import jax.numpy as jnp
from jax import lax
from jax.experimental import pallas as pl
from jax.experimental.pallas import tpu as pltpu
from jax.sharding import PartitionSpec as P

swiglu_limit = 7.0
swiglu_alpha = 1.702
norm_eps = 1e-05


def clamped_units(gate_pre, up_pre):
    capped = jnp.minimum(gate_pre, swiglu_limit)
    linear = jnp.clip(up_pre, -swiglu_limit, swiglu_limit)
    return capped * jax.nn.sigmoid(swiglu_alpha * capped) * (linear + 1.0)


def expert_work(outgoing, gate_weight, up_weight, down_weight):
    received = lax.all_to_all(outgoing, "ep", split_axis=1, concat_axis=1, tiled=True)
    local_count, sources, capacity, columns = received.shape
    row_count = sources * capacity
    row_block = received.reshape(local_count, row_count, columns)
    shard_piece = lax.all_gather(row_block, "tp", axis=2, tiled=True)
    gate_sum = jnp.einsum(
        "lrd,ldf->lrf", shard_piece, gate_weight, preferred_element_type=jnp.float32
    )
    up_sum = jnp.einsum("lrd,ldf->lrf", shard_piece, up_weight, preferred_element_type=jnp.float32)
    activation = clamped_units(gate_sum, up_sum).astype(jnp.bfloat16)
    out_cols = down_weight.shape[2]
    result = jnp.einsum(
        "lrf,lfd->lrd",
        lax.all_gather(activation, "tp", axis=2, tiled=True),
        down_weight,
        preferred_element_type=jnp.float32,
    )
    result = result.astype(jnp.bfloat16).reshape(local_count, sources, capacity, out_cols)
    return lax.all_to_all(result, "ep", split_axis=1, concat_axis=1, tiled=True)


def per_device(tokens, norm_gain, route_ids, route_weights, w_gate, w_up, w_down):
    local_count = w_gate.shape[0]
    sources = lax.axis_size("ep")
    tp_count = lax.axis_size("tp")
    width = tokens.shape[1]
    columns = width // tp_count
    experts = local_count * sources
    tok_rows, top_count = route_ids.shape
    capacity = 3 * tok_rows * top_count // (2 * experts)
    values = tokens.astype(jnp.float32)
    row_mean = jnp.mean(values, axis=1, keepdims=True)
    centred = values - row_mean
    row_var = jnp.mean(centred * centred, axis=1, keepdims=True)
    offset = lax.axis_index("tp") * columns
    own_cols = lax.dynamic_slice_in_dim(centred, offset, columns, 1)
    own_gain = lax.dynamic_slice_in_dim(norm_gain, offset, columns, 0)
    normed = (own_cols * lax.rsqrt(row_var + norm_eps) * own_gain).astype(jnp.bfloat16)
    flat_ids = route_ids.reshape(-1)
    matches = (flat_ids[:, None] == jnp.arange(experts, dtype=jnp.int32)[None, :]).astype(jnp.int32)
    earlier = jnp.cumsum(matches, axis=0) - matches
    slot_index = jnp.sum(earlier * matches, axis=1)
    position = (
        flat_ids % local_count * (sources * capacity)
        + flat_ids // local_count * capacity
        + slot_index
    )
    buffer_rows = local_count * sources * capacity
    placed = (
        position.reshape(tok_rows, top_count)[:, :, None]
        == jnp.arange(buffer_rows, dtype=jnp.int32)[None, None, :]
    )
    placement_matrix = jnp.any(placed, axis=1).astype(jnp.bfloat16)
    outgoing = jnp.einsum("tp,td->pd", placement_matrix, normed, preferred_element_type=jnp.float32)
    outgoing = outgoing.astype(jnp.bfloat16).reshape(local_count, sources, capacity, columns)
    returned = jnp.concatenate(
        [
            expert_work(
                outgoing[number : number + 1],
                w_gate[number : number + 1],
                w_up[number : number + 1],
                w_down[number : number + 1],
            )
            for number in range(local_count)
        ],
        axis=0,
    )
    flat_out = returned.reshape(buffer_rows, columns)
    picked = flat_out[position].reshape(tok_rows, top_count, columns).astype(jnp.float32)
    return jnp.sum(picked * route_weights[:, :, None], axis=1).astype(jnp.bfloat16)


CUT_SIXTEENTHS = 10
STAGES = (
    ("L", 1, 0, 0),
    ("F", 1),
    ("L", 1, 0, 1),
    ("S", 1, 0),
    ("L", 1, 1, 0),
    ("F", 2),
    ("L", 1, 1, 1),
    ("S", 1, 1),
    ("X", 2),
    ("Y", 2),
    ("L", 2, 0, 0),
    ("F", 3),
    ("L", 2, 0, 1),
    ("S", 2, 0),
    ("Y", 3),
    ("X", 3),
    ("L", 2, 1, 0),
    ("F", 4),
    ("L", 2, 1, 1),
    ("D", 2),
    ("S", 2, 1),
    ("L", 3, 0, 0),
    ("X", 4),
    ("Y", 4),
    ("F", 5),
    ("R", 2),
    ("L", 3, 0, 1),
    ("S", 3, 0),
    ("D", 3),
    ("L", 3, 1, 0),
    ("D", 4),
    ("X", 5),
    ("Y", 5),
    ("F", 6),
    ("L", 3, 1, 1),
    ("S", 3, 1),
    ("R", 4),
    ("D", 5),
    ("R", 3),
    ("X", 6),
    ("Y", 6),
    ("F", 7),
    ("R", 5),
    ("D", 6),
    ("X", 7),
    ("X", 1),
    ("Y", 7),
    ("Y", 1),
    ("X", 0),
    ("Y", 0),
    ("R", 6),
    ("D", 7),
    ("R", 7),
    ("D", 1),
    ("D", 0),
    ("R", 1),
)


def layer_kernel(
    capacity,
    tokens_hbm,
    gain_hbm,
    ids_hbm,
    mix_hbm,
    gate_hbm,
    up_hbm,
    down_hbm,
    out_ref,
    gate_w,
    up_w,
    down_w,
    tok_in,
    gain_in,
    ids_in,
    mix_in,
    toks,
    meta,
    earlier,
    rows,
    acts,
    weighted,
    combined,
    pair_out,
    pair_in,
    back_out,
    back_in,
    weight_sem,
    tok_sem,
    local_sem,
    meta_send,
    meta_recv,
    own_send,
    own_recv,
    line_send,
    line_recv,
    side_send,
    side_recv,
    mate_send,
    mate_recv,
    act_send,
    act_recv,
    pair_send,
    pair_recv,
    back_send,
    back_recv,
):
    sources = toks.shape[0]
    chips = sources // 2
    local_count = gate_w.shape[0]
    units = gate_w.shape[2]
    tok_rows = tok_in.shape[0]
    quarter = toks.shape[4]
    out_cols = down_w.shape[2]
    half_rows = tok_rows // 2
    cut = tok_rows * CUT_SIXTEENTHS // 16
    me = lax.axis_index("ep")
    tp = lax.axis_index("tp")
    z, core = me // 2, me % 2
    y, x = tp // 2, tp % 2
    tp_x = y * 2 + (1 - x)
    tp_y = (1 - y) * 2 + x
    side_tp = tp_x * (1 - core) + tp_y * core
    mate = z * 2 + (1 - core)
    own_half = (x + y) % 2
    parts = 2 if cut < tok_rows else 1

    def partner(k):
        chosen_chip = 0 * z
        for at in range(chips):
            sign = 1 if 2 * at < chips else -1
            order = sorted(range(chips), key=lambda c: (abs(c - at), sign * c))
            gap = (z - at) * (z - at)
            chosen_chip = chosen_chip + order[k] * (1 - (gap + chips * chips - 1) // (chips * chips))
        return chosen_chip

    def place(ep, column):
        return {"ep": ep, "tp": column}

    def remote(source, target, send, recv, where):
        return pltpu.make_async_remote_copy(
            src_ref=source,
            dst_ref=target,
            send_sem=send,
            recv_sem=recv,
            device_id=where,
            device_id_type=pl.DeviceIdType.MESH,
        )

    barrier = pltpu.get_barrier_semaphore()
    for d in range(1, sources):
        pl.semaphore_signal(
            barrier, inc=1, device_id=place((me + d) % sources, tp), device_id_type=pl.DeviceIdType.MESH
        )
    for column in (tp_x, tp_y):
        pl.semaphore_signal(
            barrier, inc=1, device_id=place(me, column), device_id_type=pl.DeviceIdType.MESH
        )

    piece_count = tok_sem.shape[0]
    piece_rows = tok_rows // piece_count
    tok_loads = [
        pltpu.make_async_copy(
            tokens_hbm.at[pl.ds(n * piece_rows, piece_rows)],
            tok_in.at[pl.ds(n * piece_rows, piece_rows)],
            tok_sem.at[n],
        )
        for n in range(piece_count)
    ]
    small = [
        pltpu.make_async_copy(gain_hbm, gain_in, local_sem.at[0]),
        pltpu.make_async_copy(ids_hbm, ids_in.at[me], local_sem.at[1]),
        pltpu.make_async_copy(mix_hbm, mix_in.at[me], local_sem.at[2]),
    ]
    tables = ((gate_hbm, gate_w), (up_hbm, up_w), (down_hbm, down_w))

    def load(w, n):
        hbm, vmem = tables[w]
        return pltpu.make_async_copy(hbm.at[n], vmem.at[n], weight_sem.at[w, n])

    for copy in small + tok_loads:
        copy.start()

    before = lax.broadcasted_iota(jnp.int32, (tok_rows, tok_rows), 0)
    after = lax.broadcasted_iota(jnp.int32, (tok_rows, tok_rows), 1)
    earlier[...] = (before < after).astype(jnp.float32).astype(jnp.bfloat16)

    def make_meta(source):
        ids, mix = ids_in[source], mix_in[source]
        named, scales = [], []
        for n in range(local_count):
            match = ids == me * local_count + n
            named.append(jnp.sum(match.astype(jnp.float32), axis=0, keepdims=True))
            scales.append(jnp.sum(jnp.where(match, mix, 0.0), axis=0, keepdims=True))
        pad = [jnp.zeros((1, tok_rows), jnp.float32)] * (8 - local_count)
        names = jnp.concatenate(named + pad, axis=0)
        slot = jnp.dot(names.astype(jnp.bfloat16), earlier[...], preferred_element_type=jnp.float32)
        slot = jnp.where(names > 0.0, slot, -1.0)
        meta[source, 0] = slot
        meta[source, 1] = jnp.concatenate(scales + pad, axis=0)

    for copy in small + tok_loads:
        copy.wait()
    load(0, 0).start()
    load(1, 0).start()
    band = 32

    @pl.loop(0, piece_count)
    def _(p):
        for n in range(piece_rows // band):
            at = pl.ds(pl.multiple_of(p * piece_rows + n * band, band), band)
            values = tok_in[at, :].astype(jnp.float32)
            centred = values - jnp.mean(values, axis=1, keepdims=True)
            row_var = jnp.mean(centred * centred, axis=1, keepdims=True)
            normal = (centred * lax.rsqrt(row_var + norm_eps) * gain_in[...]).astype(jnp.bfloat16)
            for q in range(4):
                toks[me, q // 2, q % 2, at, :] = normal[:, q * quarter : (q + 1) * quarter]

    for n in range(1, local_count):
        load(0, n).start()
        load(1, n).start()
    pending = []

    def go(copy):
        copy.start()
        pending.append(copy)
        return copy

    def always(condition, copy):
        pending.append((condition, copy))

    def line(chip, i, e, up):
        source = chip * 2 + i
        if e == 0:
            piece = toks.at[source, own_half, core]
        else:
            piece = toks.at[source, 1 - own_half, core, pl.ds(cut, tok_rows - cut)]
        return remote(
            piece,
            piece,
            line_send.at[up, chip, i, e],
            line_recv.at[chip, i, e],
            place((z + 2 * up - 1) * 2 + core, tp),
        )

    def side(chip, i):
        piece = toks.at[chip * 2 + i, own_half, core, pl.ds(0, cut)]
        return remote(
            piece, piece, side_send.at[chip, i], side_recv.at[chip, i], place(me, side_tp)
        )

    def to_mate(chip, i, m):
        source = chip * 2 + i
        piece = (
            toks.at[source, own_half, core],
            toks.at[source, 1 - own_half, core, pl.ds(cut, tok_rows - cut)] if parts > 1 else None,
            toks.at[source, 1 - own_half, core, pl.ds(0, cut)],
        )[m]
        return remote(
            piece, piece, mate_send.at[chip, i, m], mate_recv.at[chip, i, m], place(mate, tp)
        )

    mate_parts = (0, 1, 2) if parts > 1 else (0, 2)
    ends = ((1, z < chips - 1), (0, z > 0))

    def start_line(i):
        for e in range(parts):
            for up, there in ends:

                @pl.when(there)
                def _():
                    line(z, i, e, up).start()

    own_pieces = (
        toks.at[me, own_half, 1 - core],
        toks.at[me, 1 - own_half, 1 - core],
        toks.at[me, :, core],
    )
    own_copies = []
    metas = []

    def run_start():
        pl.semaphore_wait(barrier, sources + 1)
        for d in range(1, sources):
            for n, table in enumerate((ids_in, mix_in)):
                metas.append(
                    go(
                        remote(
                            table.at[me],
                            table.at[me],
                            meta_send.at[n, d],
                            meta_recv.at[n, d],
                            place((me + d) % sources, tp),
                        )
                    )
                )
        for n, piece in enumerate(own_pieces):
            own_copies.append(
                go(remote(piece, piece, own_send.at[n], own_recv.at[n], place(mate, tp)))
            )

        @pl.when(core == 0)
        def _():
            start_line(0)

        @pl.when(core == 1)
        def _():
            own_copies[0].wait_recv()
            own_copies[1].wait_recv()
            start_line(0)
            start_line(1)

        make_meta(me)
        compute_act(0)
        send_act(0)
        for n in range(local_count):
            load(2, n).start()

        @pl.when(core == 0)
        def _():
            own_copies[0].wait_recv()
            own_copies[1].wait_recv()
            start_line(1)

        for up, there in ends:
            for i in range(2):
                for e in range(parts):
                    always(there, line(z, i, e, up))
        for n in range(local_count):
            load(2, n).wait()

    def run_line(distance, i, e):
        for up, chip in ((1, z - distance), (0, z + distance)):
            here = chip >= 0 if up else chip < chips
            ahead = z + 2 * up - 1
            onward = jnp.logical_and(here, ahead < chips if up else ahead >= 0)

            @pl.when(here)
            def _():
                line(chip, i, e, up).wait_recv()

                @pl.when(ahead < chips if up else ahead >= 0)
                def _():
                    line(chip, i, e, up).start()

                if e == 0:
                    side(chip, i).start()
                to_mate(chip, i, e).start()

            always(onward, line(chip, i, e, up))
            if e == 0:
                always(here, side(chip, i))
            always(here, to_mate(chip, i, e))

    def run_side(k, i):
        chip = partner(k)
        side(chip, i).wait_recv()
        go(to_mate(chip, i, 2))

    def chosen(source):
        slots, scales = meta[source, 0], meta[source, 1]
        at = lax.broadcasted_iota(jnp.int32, (capacity, tok_rows), 0).astype(jnp.float32)
        hits = [at == slots[n : n + 1, :] for n in range(local_count)]
        ones = jnp.concatenate([h.astype(jnp.float32) for h in hits], axis=0)
        scale = jnp.concatenate(
            [
                jnp.sum(jnp.where(hits[n], scales[n : n + 1, :], 0.0), axis=1, keepdims=True)
                for n in range(local_count)
            ],
            axis=0,
        )
        return ones.astype(jnp.bfloat16), scale

    def source_of(s):
        if s == 0:
            return me
        if s == 1:
            return mate
        return partner(s // 2) * 2 + s % 2

    def compute_act(s):
        source = source_of(s)
        ones, _ = chosen(source)
        for q in range(4):
            got = jnp.dot(ones, toks[source, q // 2, q % 2], preferred_element_type=jnp.float32)
            got = got.astype(jnp.bfloat16)
            for n in range(local_count):
                rows[n, :, q * quarter : (q + 1) * quarter] = got[n * capacity : (n + 1) * capacity]

        @pl.loop(0, local_count)
        def _(n):
            if s == 0:
                load(0, n).wait()
                load(1, n).wait()
            block = rows[n]
            half = units // 2
            for part in range(2):
                cols = slice(part * half, (part + 1) * half)
                gate = jnp.dot(block, gate_w[n, :, cols], preferred_element_type=jnp.float32)
                up = jnp.dot(block, up_w[n, :, cols], preferred_element_type=jnp.float32)
                acts[s, tp, n, :, cols] = clamped_units(gate, up).astype(jnp.bfloat16)
            own_act(s, n, 0).start()

    def own_act(s, n, along):
        piece = acts.at[s, tp, n]
        return remote(
            piece,
            piece,
            act_send.at[s, along, n],
            act_recv.at[s, along, n],
            place(me, (tp_x, tp_y)[along]),
        )

    def passed_act(s, along):
        n = 1 - along
        piece = acts.at[s, (tp_y, tp_x)[along], n]
        return remote(
            piece,
            piece,
            act_send.at[s, along, 2],
            act_recv.at[s, along, 2],
            place(me, (tp_x, tp_y)[along]),
        )

    def send_act(s):
        for n in range(local_count):
            pending.append(own_act(s, n, 0))
        for n in reversed(range(local_count)):
            go(own_act(s, n, 1))

    def run_first(s):
        while metas:
            metas.pop().wait_recv()
        make_meta(source_of(s))
        if s == 1:
            own_copies[2].wait_recv()
        elif s > 1:
            chip = partner(s // 2)
            for m in mate_parts:
                to_mate(chip, s % 2, m).wait_recv()
        compute_act(s)
        send_act(s)

    def pass_to_y(s):
        own_act(s, 0, 0).wait_recv()
        go(passed_act(s, 1))

    def pass_to_x(s):
        own_act(s, 1, 1).wait_recv()
        go(passed_act(s, 0))

    pairs = {}

    def run_second(s):
        own_act(s, 1, 0).wait_recv()
        own_act(s, 0, 1).wait_recv()
        passed_act(s, 0).wait_recv()
        passed_act(s, 1).wait_recv()

        @pl.loop(0, local_count)
        def _(n):
            total = jnp.zeros((capacity, out_cols), jnp.float32)
            for t in range(acts.shape[1]):
                total = total + jnp.dot(
                    acts[s, t, n],
                    down_w[n, t * units : (t + 1) * units, :],
                    preferred_element_type=jnp.float32,
                )
            weighted[n] = total

        ones, scale = chosen(source_of(s))
        value = jnp.concatenate([weighted[n] for n in range(local_count)], axis=0)
        value = (value * scale).astype(jnp.bfloat16)
        result = lax.dot_general(
            ones, value, (((0,), (0,)), ((), ())), preferred_element_type=jnp.float32
        )
        for h in range(2):
            combined[s, h] = result[h * half_rows : (h + 1) * half_rows]
        if s == 1:
            for h in range(2):
                pair_out[0, h] = combined[1, h].astype(jnp.bfloat16)
            piece, target = pair_out.at[0], pair_in.at[0]
        elif s > 1:
            pair_out[s // 2, s % 2] = combined[s, 1 - core].astype(jnp.bfloat16)
            piece, target = pair_out.at[s // 2, s % 2], pair_in.at[s // 2, s % 2]
        if s > 0:
            pairs[s] = go(remote(piece, target, pair_send.at[s], pair_recv.at[s], place(mate, tp)))

    def run_back(s):
        pairs[s].wait_recv()
        if s > 1:
            k, i = s // 2, s % 2
            both = combined[s, core] + pair_in[k, i].astype(jnp.float32)
            back_out[k, i] = both.astype(jnp.bfloat16)
            go(
                remote(
                    back_out.at[k, i],
                    back_in.at[z, core],
                    back_send.at[k, i],
                    back_recv.at[z, core],
                    place(partner(k) * 2 + i, tp),
                )
            )

    run_start()
    runs = {
        "L": run_line,
        "S": run_side,
        "F": run_first,
        "X": pass_to_y,
        "Y": pass_to_x,
        "D": run_second,
        "R": run_back,
    }
    for kind, *rest in STAGES:
        runs[kind](*rest)
    for h in range(2):
        result = combined[0, h] + pair_in[0, h].astype(jnp.float32)
        for d in range(1, chips):
            chip = (z + d) % chips
            remote(
                back_out.at[0, 0], back_in.at[chip, h], back_send.at[0, h], back_recv.at[chip, h], place(mate, tp)
            ).wait_recv()
            result = result + back_in[chip, h].astype(jnp.float32)
        out_ref[h * half_rows : (h + 1) * half_rows, :] = result.astype(out_ref.dtype)
    for entry in pending:
        if isinstance(entry, tuple):

            @pl.when(entry[0])
            def _():
                entry[1].wait_send()
        else:
            entry.wait_send()


def fused_per_device(tokens, norm_gain, route_ids, route_weights, w_gate, w_up, w_down):
    local_count, width, units = w_gate.shape
    out_cols = w_down.shape[2]
    sources = lax.axis_size("ep")
    tp_count = lax.axis_size("tp")
    experts = local_count * sources
    tok_rows, top_count = route_ids.shape
    capacity = 3 * tok_rows * top_count // (2 * experts)
    chips = sources // 2
    quarter = width // 4
    half_rows = tok_rows // 2
    dma = pltpu.SemaphoreType.DMA
    bf16 = jnp.bfloat16
    vmem = pl.BlockSpec(memory_space=pltpu.VMEM)
    hbm = pl.BlockSpec(memory_space=pltpu.HBM)
    return pl.pallas_call(
        functools.partial(layer_kernel, capacity),
        out_shape=jax.ShapeDtypeStruct((tok_rows, out_cols), bf16),
        in_specs=[hbm] * 7,
        out_specs=vmem,
        scratch_shapes=[
            pltpu.VMEM(w_gate.shape, bf16),
            pltpu.VMEM(w_up.shape, bf16),
            pltpu.VMEM(w_down.shape, bf16),
            pltpu.VMEM(tokens.shape, bf16),
            pltpu.VMEM((1, width), jnp.float32),
            pltpu.VMEM((sources, top_count, tok_rows), jnp.int32),
            pltpu.VMEM((sources, top_count, tok_rows), jnp.float32),
            pltpu.VMEM((sources, 2, 2, tok_rows, quarter), bf16),
            pltpu.VMEM((sources, 2, 8, tok_rows), jnp.float32),
            pltpu.VMEM((tok_rows, tok_rows), bf16),
            pltpu.VMEM((local_count, capacity, width), bf16),
            pltpu.VMEM((sources, tp_count, local_count, capacity, units), bf16),
            pltpu.VMEM((local_count, capacity, out_cols), jnp.float32),
            pltpu.VMEM((sources, 2, half_rows, out_cols), jnp.float32),
            pltpu.VMEM((chips, 2, half_rows, out_cols), bf16),
            pltpu.VMEM((chips, 2, half_rows, out_cols), bf16),
            pltpu.VMEM((chips, 2, half_rows, out_cols), bf16),
            pltpu.VMEM((chips, 2, half_rows, out_cols), bf16),
            dma((3, local_count)),
            dma((4,)),
            dma((3,)),
            dma((2, sources)),
            dma((2, sources)),
            dma((3,)),
            dma((3,)),
            dma((2, chips, 2, 2)),
            dma((chips, 2, 2)),
            dma((chips, 2)),
            dma((chips, 2)),
            dma((chips, 2, 3)),
            dma((chips, 2, 3)),
            dma((sources, 2, 3)),
            dma((sources, 2, 3)),
            dma((sources,)),
            dma((sources,)),
            dma((chips, 2)),
            dma((chips, 2)),
        ],
        compiler_params=pltpu.CompilerParams(
            collective_id=0, has_side_effects=True, vmem_limit_bytes=60 * 1024 * 1024
        ),
    )(tokens, norm_gain.reshape(1, width), route_ids.T, route_weights.T, w_gate, w_up, w_down)


def pick_plan(mesh):
    sources, tp_count = mesh.shape["ep"], mesh.shape["tp"]

    def body(tokens, norm_gain, route_ids, route_weights, w_gate, w_up, w_down):
        tok_rows, top_count = route_ids.shape
        experts = w_gate.shape[0] * sources
        capacity = 3 * tok_rows * top_count // (2 * experts)
        gathered = 2 * tokens.size * sources + 6 * w_gate.size
        fused = (
            tp_count == 4
            and sources == 8
            and capacity % 16 == 0
            and w_gate.shape[0] == 2
            and tok_rows % 128 == 0
            and tokens.shape[1] % 512 == 0
            and gathered < 32 * 1024 * 1024
        )
        run = fused_per_device if fused else per_device
        return run(tokens, norm_gain, route_ids, route_weights, w_gate, w_up, w_down)

    return body


def solution(mesh):
    return jax.shard_map(
        pick_plan(mesh),
        mesh=mesh,
        in_specs=(
            P("ep", None),
            P(),
            P("ep", None),
            P("ep", None),
            P("ep", None, "tp"),
            P("ep", None, "tp"),
            P("ep", None, "tp"),
        ),
        out_specs=P("ep", "tp"),
        check_vma=False,
    )
```

```python
import functools
import jax
import jax.numpy as jnp
from jax import lax
from jax.experimental import pallas as pl
from jax.experimental.pallas import tpu as pltpu
from jax.sharding import PartitionSpec as P

swiglu_limit = 7.0
swiglu_alpha = 1.702
norm_eps = 1e-05


def clamped_units(gate_pre, up_pre):
    capped = jnp.minimum(gate_pre, swiglu_limit)
    linear = jnp.clip(up_pre, -swiglu_limit, swiglu_limit)
    return capped * jax.nn.sigmoid(swiglu_alpha * capped) * (linear + 1.0)


def expert_work(outgoing, gate_weight, up_weight, down_weight):
    received = lax.all_to_all(outgoing, "ep", split_axis=1, concat_axis=1, tiled=True)
    local_count, sources, capacity, columns = received.shape
    row_count = sources * capacity
    row_block = received.reshape(local_count, row_count, columns)
    shard_piece = lax.all_gather(row_block, "tp", axis=2, tiled=True)
    gate_sum = jnp.einsum(
        "lrd,ldf->lrf", shard_piece, gate_weight, preferred_element_type=jnp.float32
    )
    up_sum = jnp.einsum("lrd,ldf->lrf", shard_piece, up_weight, preferred_element_type=jnp.float32)
    activation = clamped_units(gate_sum, up_sum).astype(jnp.bfloat16)
    out_cols = down_weight.shape[2]
    result = jnp.einsum(
        "lrf,lfd->lrd",
        lax.all_gather(activation, "tp", axis=2, tiled=True),
        down_weight,
        preferred_element_type=jnp.float32,
    )
    result = result.astype(jnp.bfloat16).reshape(local_count, sources, capacity, out_cols)
    return lax.all_to_all(result, "ep", split_axis=1, concat_axis=1, tiled=True)


def per_device(tokens, norm_gain, route_ids, route_weights, w_gate, w_up, w_down):
    local_count = w_gate.shape[0]
    sources = lax.axis_size("ep")
    tp_count = lax.axis_size("tp")
    width = tokens.shape[1]
    columns = width // tp_count
    experts = local_count * sources
    tok_rows, top_count = route_ids.shape
    capacity = 3 * tok_rows * top_count // (2 * experts)
    values = tokens.astype(jnp.float32)
    row_mean = jnp.mean(values, axis=1, keepdims=True)
    centred = values - row_mean
    row_var = jnp.mean(centred * centred, axis=1, keepdims=True)
    offset = lax.axis_index("tp") * columns
    own_cols = lax.dynamic_slice_in_dim(centred, offset, columns, 1)
    own_gain = lax.dynamic_slice_in_dim(norm_gain, offset, columns, 0)
    normed = (own_cols * lax.rsqrt(row_var + norm_eps) * own_gain).astype(jnp.bfloat16)
    flat_ids = route_ids.reshape(-1)
    matches = (flat_ids[:, None] == jnp.arange(experts, dtype=jnp.int32)[None, :]).astype(jnp.int32)
    earlier = jnp.cumsum(matches, axis=0) - matches
    slot_index = jnp.sum(earlier * matches, axis=1)
    position = (
        flat_ids % local_count * (sources * capacity)
        + flat_ids // local_count * capacity
        + slot_index
    )
    buffer_rows = local_count * sources * capacity
    placed = (
        position.reshape(tok_rows, top_count)[:, :, None]
        == jnp.arange(buffer_rows, dtype=jnp.int32)[None, None, :]
    )
    placement_matrix = jnp.any(placed, axis=1).astype(jnp.bfloat16)
    outgoing = jnp.einsum("tp,td->pd", placement_matrix, normed, preferred_element_type=jnp.float32)
    outgoing = outgoing.astype(jnp.bfloat16).reshape(local_count, sources, capacity, columns)
    returned = jnp.concatenate(
        [
            expert_work(
                outgoing[number : number + 1],
                w_gate[number : number + 1],
                w_up[number : number + 1],
                w_down[number : number + 1],
            )
            for number in range(local_count)
        ],
        axis=0,
    )
    flat_out = returned.reshape(buffer_rows, columns)
    picked = flat_out[position].reshape(tok_rows, top_count, columns).astype(jnp.float32)
    return jnp.sum(picked * route_weights[:, :, None], axis=1).astype(jnp.bfloat16)


CUT_SIXTEENTHS = 10
STAGES = (
    ("L", 1, 0, 0),
    ("F", 1),
    ("L", 1, 0, 1),
    ("S", 1, 0),
    ("L", 1, 1, 0),
    ("F", 2),
    ("L", 1, 1, 1),
    ("S", 1, 1),
    ("X", 2),
    ("Y", 2),
    ("L", 2, 0, 0),
    ("F", 3),
    ("L", 2, 0, 1),
    ("S", 2, 0),
    ("Y", 3),
    ("X", 3),
    ("L", 2, 1, 0),
    ("F", 4),
    ("L", 2, 1, 1),
    ("D", 2),
    ("S", 2, 1),
    ("L", 3, 0, 0),
    ("X", 4),
    ("Y", 4),
    ("F", 5),
    ("R", 2),
    ("L", 3, 0, 1),
    ("S", 3, 0),
    ("D", 3),
    ("L", 3, 1, 0),
    ("D", 4),
    ("X", 5),
    ("Y", 5),
    ("F", 6),
    ("L", 3, 1, 1),
    ("S", 3, 1),
    ("R", 4),
    ("D", 5),
    ("R", 3),
    ("X", 6),
    ("Y", 6),
    ("F", 7),
    ("R", 5),
    ("D", 6),
    ("X", 7),
    ("X", 1),
    ("Y", 7),
    ("Y", 1),
    ("X", 0),
    ("Y", 0),
    ("R", 6),
    ("D", 7),
    ("R", 7),
    ("D", 1),
    ("D", 0),
    ("R", 1),
)


def layer_kernel(
    capacity,
    tokens_hbm,
    gain_hbm,
    ids_hbm,
    mix_hbm,
    gate_hbm,
    up_hbm,
    down_hbm,
    out_ref,
    gate_w,
    up_w,
    down_w,
    tok_in,
    gain_in,
    ids_in,
    mix_in,
    toks,
    meta,
    earlier,
    rows,
    acts,
    weighted,
    combined,
    pair_out,
    pair_in,
    back_out,
    back_in,
    weight_sem,
    tok_sem,
    local_sem,
    meta_send,
    meta_recv,
    own_recv,
    line_send,
    line_recv,
    side_send,
    side_recv,
    mate_send,
    mate_recv,
    act_send,
    act_recv,
    pair_send,
    pair_recv,
    back_send,
    back_recv,
):
    sources = toks.shape[0]
    chips = sources // 2
    local_count = gate_w.shape[0]
    units = gate_w.shape[2]
    tok_rows = tok_in.shape[0]
    quarter = toks.shape[4]
    out_cols = down_w.shape[2]
    half_rows = tok_rows // 2
    cut = tok_rows * CUT_SIXTEENTHS // 16
    me = lax.axis_index("ep")
    tp = lax.axis_index("tp")
    z, core = me // 2, me % 2
    y, x = tp // 2, tp % 2
    tp_x = y * 2 + (1 - x)
    tp_y = (1 - y) * 2 + x
    side_tp = tp_x * (1 - core) + tp_y * core
    mate = z * 2 + (1 - core)
    own_half = (x + y) % 2
    parts = 2 if cut < tok_rows else 1

    def partner(k):
        chosen_chip = 0 * z
        for at in range(chips):
            sign = 1 if 2 * at < chips else -1
            order = sorted(range(chips), key=lambda c: (abs(c - at), sign * c))
            gap = (z - at) * (z - at)
            chosen_chip = chosen_chip + order[k] * (1 - (gap + chips * chips - 1) // (chips * chips))
        return chosen_chip

    def place(ep, column):
        return {"ep": ep, "tp": column}

    def remote(source, target, send, recv, where):
        return pltpu.make_async_remote_copy(
            src_ref=source,
            dst_ref=target,
            send_sem=send,
            recv_sem=recv,
            device_id=where,
            device_id_type=pl.DeviceIdType.MESH,
        )

    barrier = pltpu.get_barrier_semaphore()
    for d in range(1, sources):
        pl.semaphore_signal(
            barrier, inc=1, device_id=place((me + d) % sources, tp), device_id_type=pl.DeviceIdType.MESH
        )
    for column in (tp_x, tp_y):
        pl.semaphore_signal(
            barrier, inc=1, device_id=place(me, column), device_id_type=pl.DeviceIdType.MESH
        )

    tok_loads = [pltpu.make_async_copy(tokens_hbm, tok_in, tok_sem.at[0])]
    small = [
        pltpu.make_async_copy(gain_hbm, gain_in, local_sem.at[0]),
        pltpu.make_async_copy(ids_hbm, ids_in.at[me], local_sem.at[1]),
        pltpu.make_async_copy(mix_hbm, mix_in.at[me], local_sem.at[2]),
    ]
    tables = ((gate_hbm, gate_w), (up_hbm, up_w), (down_hbm, down_w))

    def load(w, n):
        hbm, vmem = tables[w]
        return pltpu.make_async_copy(hbm.at[n], vmem.at[n], weight_sem.at[w, n])

    for copy in small + tok_loads:
        copy.start()

    before = lax.broadcasted_iota(jnp.int32, (tok_rows, tok_rows), 0)
    after = lax.broadcasted_iota(jnp.int32, (tok_rows, tok_rows), 1)
    earlier[...] = (before < after).astype(jnp.float32).astype(jnp.bfloat16)

    def make_meta(source):
        ids, mix = ids_in[source], mix_in[source]
        named, scales = [], []
        for n in range(local_count):
            match = ids == me * local_count + n
            named.append(jnp.sum(match.astype(jnp.float32), axis=0, keepdims=True))
            scales.append(jnp.sum(jnp.where(match, mix, 0.0), axis=0, keepdims=True))
        pad = [jnp.zeros((1, tok_rows), jnp.float32)] * (8 - local_count)
        names = jnp.concatenate(named + pad, axis=0)
        slot = jnp.dot(names.astype(jnp.bfloat16), earlier[...], preferred_element_type=jnp.float32)
        slot = jnp.where(names > 0.0, slot, -1.0)
        meta[source, 0] = slot
        meta[source, 1] = jnp.concatenate(scales + pad, axis=0)

    for copy in small + tok_loads:
        copy.wait()
    load(0, 0).start()
    load(1, 0).start()
    band = 32

    @pl.loop(0, tok_rows // (2 * band))
    def _(p):
        for n in range(2):
            at = pl.ds(pl.multiple_of((2 * p + n) * band, band), band)
            values = tok_in[at, :].astype(jnp.float32)
            centred = values - jnp.mean(values, axis=1, keepdims=True)
            row_var = jnp.mean(centred * centred, axis=1, keepdims=True)
            normal = (centred * lax.rsqrt(row_var + norm_eps) * gain_in[...]).astype(jnp.bfloat16)
            for q in range(4):
                toks[me, q // 2, q % 2, at, :] = normal[:, q * quarter : (q + 1) * quarter]

    for n in range(1, local_count):
        load(0, n).start()
        load(1, n).start()
    def go(copy):
        copy.start()
        return copy

    def all_sent(piece, semaphore):
        remote(piece, piece, semaphore, back_recv.at[0], place(mate, tp)).wait_send()

    def all_here(piece, semaphore):
        remote(piece, piece, back_send.at[0], semaphore, place(mate, tp)).wait_recv()

    def line(chip, i, e, up):
        source = chip * 2 + i
        if e == 0:
            piece = toks.at[source, own_half, core]
        else:
            piece = toks.at[source, 1 - own_half, core, pl.ds(cut, tok_rows - cut)]
        return remote(
            piece,
            piece,
            line_send.at[up, e],
            line_recv.at[chip, i, e],
            place((z + 2 * up - 1) * 2 + core, tp),
        )

    def side(chip, i):
        piece = toks.at[chip * 2 + i, own_half, core, pl.ds(0, cut)]
        return remote(
            piece, piece, side_send.at[0], side_recv.at[chip, i], place(me, side_tp)
        )

    def to_mate(chip, i, m):
        source = chip * 2 + i
        piece = (
            toks.at[source, own_half, core],
            toks.at[source, 1 - own_half, core, pl.ds(cut, tok_rows - cut)] if parts > 1 else None,
            toks.at[source, 1 - own_half, core, pl.ds(0, cut)],
        )[m]
        return remote(
            piece, piece, mate_send.at[0], mate_recv.at[chip, i], place(mate, tp)
        )

    ends = ((1, z < chips - 1), (0, z > 0))

    def start_line(i):
        for e in range(parts):
            for up, there in ends:

                @pl.when(there)
                def _():
                    line(z, i, e, up).start()

    own_pieces = (
        toks.at[me, own_half, 1 - core],
        toks.at[me, 1 - own_half, 1 - core],
        toks.at[me, :, core],
    )
    own_copies = []
    metas = []

    def run_start():
        pl.semaphore_wait(barrier, sources + 1)
        for d in range(1, sources):
            for n, table in enumerate((ids_in, mix_in)):
                metas.append(
                    go(
                        remote(
                            table.at[me],
                            table.at[me],
                            meta_send.at[n],
                            meta_recv.at[n],
                            place((me + d) % sources, tp),
                        )
                    )
                )
        for n, piece in enumerate(own_pieces):
            own_copies.append(
                go(remote(piece, piece, mate_send.at[0], own_recv.at[n], place(mate, tp)))
            )

        @pl.when(core == 0)
        def _():
            start_line(0)

        @pl.when(core == 1)
        def _():
            own_copies[0].wait_recv()
            own_copies[1].wait_recv()
            start_line(0)
            start_line(1)

        make_meta(me)
        compute_act(0)
        send_act(0)
        for n in range(local_count):
            load(2, n).start()

        @pl.when(core == 0)
        def _():
            own_copies[0].wait_recv()
            own_copies[1].wait_recv()
            start_line(1)

        for n in range(local_count):
            load(2, n).wait()

    def run_line(distance, i, e):
        for up, chip in ((1, z - distance), (0, z + distance)):
            here = chip >= 0 if up else chip < chips
            ahead = z + 2 * up - 1

            @pl.when(here)
            def _():
                line(chip, i, e, up).wait_recv()

                @pl.when(ahead < chips if up else ahead >= 0)
                def _():
                    line(chip, i, e, up).start()

                if e == 0:
                    side(chip, i).start()
                to_mate(chip, i, e).start()


    def run_side(k, i):
        chip = partner(k)
        side(chip, i).wait_recv()
        go(to_mate(chip, i, 2))

    def chosen(source):
        slots, scales = meta[source, 0], meta[source, 1]
        at = lax.broadcasted_iota(jnp.int32, (capacity, tok_rows), 0).astype(jnp.float32)
        hits = [at == slots[n : n + 1, :] for n in range(local_count)]
        ones = jnp.concatenate([h.astype(jnp.float32) for h in hits], axis=0)
        scale = jnp.concatenate(
            [
                jnp.sum(jnp.where(hits[n], scales[n : n + 1, :], 0.0), axis=1, keepdims=True)
                for n in range(local_count)
            ],
            axis=0,
        )
        return ones.astype(jnp.bfloat16), scale

    def source_of(s):
        if s == 0:
            return me
        if s == 1:
            return mate
        return partner(s // 2) * 2 + s % 2

    def compute_act(s):
        source = source_of(s)
        ones, _ = chosen(source)
        for q in range(4):
            got = jnp.dot(ones, toks[source, q // 2, q % 2], preferred_element_type=jnp.float32)
            got = got.astype(jnp.bfloat16)
            for n in range(local_count):
                rows[n, :, q * quarter : (q + 1) * quarter] = got[n * capacity : (n + 1) * capacity]

        @pl.loop(0, local_count)
        def _(n):
            if s == 0:
                load(0, n).wait()
                load(1, n).wait()
            block = rows[n]
            half = units // 2
            for part in range(2):
                cols = slice(part * half, (part + 1) * half)
                gate = jnp.dot(block, gate_w[n, :, cols], preferred_element_type=jnp.float32)
                up = jnp.dot(block, up_w[n, :, cols], preferred_element_type=jnp.float32)
                acts[s, tp, n, :, cols] = clamped_units(gate, up).astype(jnp.bfloat16)
            own_act(s, n, 0).start()

    def own_act(s, n, along):
        piece = acts.at[s, tp, n]
        return remote(
            piece,
            piece,
            act_send.at[0],
            act_recv.at[s, 2 - (2 - along) * (1 - (n - along) * (n - along))],
            place(me, (tp_x, tp_y)[along]),
        )

    def passed_act(s, along):
        n = 1 - along
        piece = acts.at[s, (tp_y, tp_x)[along], n]
        return remote(
            piece,
            piece,
            act_send.at[0],
            act_recv.at[s, 2],
            place(me, (tp_x, tp_y)[along]),
        )

    def send_act(s):
        for n in reversed(range(local_count)):
            go(own_act(s, n, 1))

    def run_first(s):
        if metas:
            all_here(ids_in.at[pl.ds(0, sources - 1)], meta_recv.at[0])
            all_here(mix_in.at[pl.ds(0, sources - 1)], meta_recv.at[1])
            metas.clear()
        make_meta(source_of(s))
        if s == 1:
            own_copies[2].wait_recv()
        elif s > 1:
            chip = partner(s // 2)
            all_here(toks.at[chip * 2 + s % 2, :, core], mate_recv.at[chip, s % 2])
        compute_act(s)
        send_act(s)

    def pass_to_y(s):
        own_act(s, 0, 0).wait_recv()
        go(passed_act(s, 1))

    def pass_to_x(s):
        own_act(s, 1, 1).wait_recv()
        go(passed_act(s, 0))

    pairs = {}

    def run_second(s):
        all_here(acts.at[s, pl.ds(0, 2)], act_recv.at[s, 2])

        @pl.loop(0, local_count)
        def _(n):
            total = jnp.zeros((capacity, out_cols), jnp.float32)
            for t in range(acts.shape[1]):
                total = total + jnp.dot(
                    acts[s, t, n],
                    down_w[n, t * units : (t + 1) * units, :],
                    preferred_element_type=jnp.float32,
                )
            weighted[n] = total

        ones, scale = chosen(source_of(s))
        value = jnp.concatenate([weighted[n] for n in range(local_count)], axis=0)
        value = (value * scale).astype(jnp.bfloat16)
        result = lax.dot_general(
            ones, value, (((0,), (0,)), ((), ())), preferred_element_type=jnp.float32
        )
        for h in range(2):
            combined[s, h] = result[h * half_rows : (h + 1) * half_rows]
        if s == 1:
            for h in range(2):
                pair_out[0, h] = combined[1, h].astype(jnp.bfloat16)
            piece, target = pair_out.at[0], pair_in.at[0]
        elif s > 1:
            pair_out[s // 2, s % 2] = combined[s, 1 - core].astype(jnp.bfloat16)
            piece, target = pair_out.at[s // 2, s % 2], pair_in.at[s // 2, s % 2]
        if s > 0:
            pairs[s] = go(remote(piece, target, pair_send.at[0], pair_recv.at[s], place(mate, tp)))

    def run_back(s):
        pairs[s].wait_recv()
        if s > 1:
            k, i = s // 2, s % 2
            both = combined[s, core] + pair_in[k, i].astype(jnp.float32)
            back_out[k, i] = both.astype(jnp.bfloat16)
            go(
                remote(
                    back_out.at[k, i],
                    back_in.at[z, core],
                    back_send.at[0],
                    back_recv.at[0],
                    place(partner(k) * 2 + i, tp),
                )
            )

    run_start()
    runs = {
        "L": run_line,
        "S": run_side,
        "F": run_first,
        "X": pass_to_y,
        "Y": pass_to_x,
        "D": run_second,
        "R": run_back,
    }
    for kind, *rest in STAGES:
        runs[kind](*rest)
    all_here(back_in.at[pl.ds(0, chips - 1)], back_recv.at[0])
    for h in range(2):
        result = combined[0, h] + pair_in[0, h].astype(jnp.float32)
        for d in range(1, chips):
            result = result + back_in[(z + d) % chips, h].astype(jnp.float32)
        out_ref[h * half_rows : (h + 1) * half_rows, :] = result.astype(out_ref.dtype)
    all_sent(ids_in.at[pl.ds(0, sources - 1)], meta_send.at[0])
    all_sent(mix_in.at[pl.ds(0, sources - 1)], meta_send.at[1])
    all_sent(toks.at[pl.ds(0, chips)], mate_send.at[0])
    all_sent(toks.at[pl.ds(0, 2 * chips - 2), 0, 0, pl.ds(0, cut)], side_send.at[0])
    all_sent(acts.at[pl.ds(0, 3 * sources // 4)], act_send.at[0])
    all_sent(pair_out, pair_send.at[0])
    all_sent(back_out.at[pl.ds(1, chips - 1)], back_send.at[0])
    for at in range(chips):

        @pl.when(z == at)
        def _():
            for up, chip_count in ((1, at + 1), (0, chips - at)):
                if chip_count == chips:
                    continue
                for e in range(parts):
                    first, size = ((0, tok_rows), (cut, tok_rows - cut))[e]
                    all_sent(
                        toks.at[pl.ds(0, 2 * chip_count), 0, 0, pl.ds(first, size)],
                        line_send.at[up, e],
                    )


def fused_per_device(tokens, norm_gain, route_ids, route_weights, w_gate, w_up, w_down):
    local_count, width, units = w_gate.shape
    out_cols = w_down.shape[2]
    sources = lax.axis_size("ep")
    tp_count = lax.axis_size("tp")
    experts = local_count * sources
    tok_rows, top_count = route_ids.shape
    capacity = 3 * tok_rows * top_count // (2 * experts)
    chips = sources // 2
    quarter = width // 4
    half_rows = tok_rows // 2
    dma = pltpu.SemaphoreType.DMA
    bf16 = jnp.bfloat16
    vmem = pl.BlockSpec(memory_space=pltpu.VMEM)
    hbm = pl.BlockSpec(memory_space=pltpu.HBM)
    return pl.pallas_call(
        functools.partial(layer_kernel, capacity),
        out_shape=pltpu.VMEM((tok_rows, out_cols), bf16),
        in_specs=[hbm] * 7,
        out_specs=vmem,
        scratch_shapes=[
            pltpu.VMEM(w_gate.shape, bf16),
            pltpu.VMEM(w_up.shape, bf16),
            pltpu.VMEM(w_down.shape, bf16),
            pltpu.VMEM(tokens.shape, bf16),
            pltpu.VMEM((1, width), jnp.float32),
            pltpu.VMEM((sources, top_count, tok_rows), jnp.int32),
            pltpu.VMEM((sources, top_count, tok_rows), jnp.float32),
            pltpu.VMEM((sources, 2, 2, tok_rows, quarter), bf16),
            pltpu.VMEM((sources, 2, 8, tok_rows), jnp.float32),
            pltpu.VMEM((tok_rows, tok_rows), bf16),
            pltpu.VMEM((local_count, capacity, width), bf16),
            pltpu.VMEM((sources, tp_count, local_count, capacity, units), bf16),
            pltpu.VMEM((local_count, capacity, out_cols), jnp.float32),
            pltpu.VMEM((sources, 2, half_rows, out_cols), jnp.float32),
            pltpu.VMEM((chips, 2, half_rows, out_cols), bf16),
            pltpu.VMEM((chips, 2, half_rows, out_cols), bf16),
            pltpu.VMEM((chips, 2, half_rows, out_cols), bf16),
            pltpu.VMEM((chips, 2, half_rows, out_cols), bf16),
            dma((3, local_count)),
            dma((1,)),
            dma((3,)),
            dma((2,)),
            dma((2,)),
            dma((3,)),
            dma((2, 2)),
            dma((chips, 2, 2)),
            dma((1,)),
            dma((chips, 2)),
            dma((1,)),
            dma((chips, 2)),
            dma((1,)),
            dma((sources, 3)),
            dma((1,)),
            dma((sources,)),
            dma((1,)),
            dma((1,)),
        ],
        compiler_params=pltpu.CompilerParams(
            collective_id=0, has_side_effects=True, vmem_limit_bytes=61 * 1024 * 1024
        ),
    )(tokens, norm_gain.reshape(1, width), route_ids.T, route_weights.T, w_gate, w_up, w_down)


def pick_plan(mesh):
    sources, tp_count = mesh.shape["ep"], mesh.shape["tp"]

    def body(tokens, norm_gain, route_ids, route_weights, w_gate, w_up, w_down):
        tok_rows, top_count = route_ids.shape
        experts = w_gate.shape[0] * sources
        capacity = 3 * tok_rows * top_count // (2 * experts)
        gathered = 2 * tokens.size * sources + 6 * w_gate.size
        fused = (
            tp_count == 4
            and sources == 8
            and capacity % 16 == 0
            and w_gate.shape[0] == 2
            and tok_rows % 128 == 0
            and tokens.shape[1] % 512 == 0
            and gathered < 32 * 1024 * 1024
        )
        run = fused_per_device if fused else per_device
        return run(tokens, norm_gain, route_ids, route_weights, w_gate, w_up, w_down)

    return body


def solution(mesh):
    return jax.shard_map(
        pick_plan(mesh),
        mesh=mesh,
        in_specs=(
            P("ep", None),
            P(),
            P("ep", None),
            P("ep", None),
            P("ep", None, "tp"),
            P("ep", None, "tp"),
            P("ep", None, "tp"),
        ),
        out_specs=P("ep", "tp"),
        check_vma=False,
    )
```

```python
import functools
import jax
import jax.numpy as jnp
from jax import lax
from jax.experimental import pallas as pl
from jax.experimental.pallas import tpu as pltpu
from jax.sharding import PartitionSpec as P

swiglu_limit = 7.0
swiglu_alpha = 1.702
norm_eps = 1e-05


def clamped_units(gate_pre, up_pre):
    capped = jnp.minimum(gate_pre, swiglu_limit)
    linear = jnp.clip(up_pre, -swiglu_limit, swiglu_limit)
    return capped * jax.nn.sigmoid(swiglu_alpha * capped) * (linear + 1.0)


def expert_work(outgoing, gate_weight, up_weight, down_weight):
    received = lax.all_to_all(outgoing, "ep", split_axis=1, concat_axis=1, tiled=True)
    local_count, sources, capacity, columns = received.shape
    row_count = sources * capacity
    row_block = received.reshape(local_count, row_count, columns)
    shard_piece = lax.all_gather(row_block, "tp", axis=2, tiled=True)
    gate_sum = jnp.einsum(
        "lrd,ldf->lrf", shard_piece, gate_weight, preferred_element_type=jnp.float32
    )
    up_sum = jnp.einsum("lrd,ldf->lrf", shard_piece, up_weight, preferred_element_type=jnp.float32)
    activation = clamped_units(gate_sum, up_sum).astype(jnp.bfloat16)
    out_cols = down_weight.shape[2]
    result = jnp.einsum(
        "lrf,lfd->lrd",
        lax.all_gather(activation, "tp", axis=2, tiled=True),
        down_weight,
        preferred_element_type=jnp.float32,
    )
    result = result.astype(jnp.bfloat16).reshape(local_count, sources, capacity, out_cols)
    return lax.all_to_all(result, "ep", split_axis=1, concat_axis=1, tiled=True)


def per_device(tokens, norm_gain, route_ids, route_weights, w_gate, w_up, w_down):
    local_count = w_gate.shape[0]
    sources = lax.axis_size("ep")
    tp_count = lax.axis_size("tp")
    width = tokens.shape[1]
    columns = width // tp_count
    experts = local_count * sources
    tok_rows, top_count = route_ids.shape
    capacity = 3 * tok_rows * top_count // (2 * experts)
    values = tokens.astype(jnp.float32)
    row_mean = jnp.mean(values, axis=1, keepdims=True)
    centred = values - row_mean
    row_var = jnp.mean(centred * centred, axis=1, keepdims=True)
    offset = lax.axis_index("tp") * columns
    own_cols = lax.dynamic_slice_in_dim(centred, offset, columns, 1)
    own_gain = lax.dynamic_slice_in_dim(norm_gain, offset, columns, 0)
    normed = (own_cols * lax.rsqrt(row_var + norm_eps) * own_gain).astype(jnp.bfloat16)
    flat_ids = route_ids.reshape(-1)
    matches = (flat_ids[:, None] == jnp.arange(experts, dtype=jnp.int32)[None, :]).astype(jnp.int32)
    earlier = jnp.cumsum(matches, axis=0) - matches
    slot_index = jnp.sum(earlier * matches, axis=1)
    position = (
        flat_ids % local_count * (sources * capacity)
        + flat_ids // local_count * capacity
        + slot_index
    )
    buffer_rows = local_count * sources * capacity
    placed = (
        position.reshape(tok_rows, top_count)[:, :, None]
        == jnp.arange(buffer_rows, dtype=jnp.int32)[None, None, :]
    )
    placement_matrix = jnp.any(placed, axis=1).astype(jnp.bfloat16)
    outgoing = jnp.einsum("tp,td->pd", placement_matrix, normed, preferred_element_type=jnp.float32)
    outgoing = outgoing.astype(jnp.bfloat16).reshape(local_count, sources, capacity, columns)
    returned = jnp.concatenate(
        [
            expert_work(
                outgoing[number : number + 1],
                w_gate[number : number + 1],
                w_up[number : number + 1],
                w_down[number : number + 1],
            )
            for number in range(local_count)
        ],
        axis=0,
    )
    flat_out = returned.reshape(buffer_rows, columns)
    picked = flat_out[position].reshape(tok_rows, top_count, columns).astype(jnp.float32)
    return jnp.sum(picked * route_weights[:, :, None], axis=1).astype(jnp.bfloat16)


CUT_SIXTEENTHS = 10
STAGES = (
    ("Y", 0),
    ("L", 1, 0, 0),
    ("F", 1),
    ("L", 1, 0, 1),
    ("X", 0),
    ("S", 1, 0),
    ("Y", 1),
    ("L", 1, 1, 0),
    ("F", 2),
    ("L", 1, 1, 1),
    ("S", 1, 1),
    ("Y", 2),
    ("X", 2),
    ("L", 2, 0, 0),
    ("F", 3),
    ("L", 2, 0, 1),
    ("S", 2, 0),
    ("Y", 3),
    ("X", 3),
    ("L", 2, 1, 0),
    ("F", 4),
    ("D", 2),
    ("D", 3),
    ("L", 2, 1, 1),
    ("S", 2, 1),
    ("L", 3, 0, 0),
    ("Y", 4),
    ("X", 4),
    ("F", 5),
    ("R", 3),
    ("L", 3, 0, 1),
    ("D", 0),
    ("S", 3, 0),
    ("X", 5),
    ("Y", 5),
    ("L", 3, 1, 0),
    ("D", 4),
    ("F", 6),
    ("R", 4),
    ("L", 3, 1, 1),
    ("D", 5),
    ("S", 3, 1),
    ("R", 5),
    ("Y", 6),
    ("X", 6),
    ("F", 7),
    ("D", 6),
    ("X", 7),
    ("X", 1),
    ("Y", 7),
    ("R", 6),
    ("R", 2),
    ("D", 7),
    ("R", 7),
    ("D", 1),
    ("R", 1),
)


def layer_kernel(
    capacity,
    tokens_hbm,
    gain_hbm,
    ids_hbm,
    mix_hbm,
    gate_hbm,
    up_hbm,
    down_hbm,
    out_ref,
    gate_w,
    up_w,
    down_w,
    tok_in,
    gain_in,
    ids_in,
    mix_in,
    toks,
    meta,
    earlier,
    rows,
    acts,
    weighted,
    combined,
    pair_out,
    pair_in,
    back_out,
    back_in,
    weight_sem,
    tok_sem,
    local_sem,
    meta_send,
    meta_recv,
    own_recv,
    line_send,
    line_recv,
    side_send,
    side_recv,
    mate_send,
    mate_recv,
    act_send,
    act_recv,
    pair_send,
    pair_recv,
    back_send,
    back_recv,
):
    sources = toks.shape[0]
    chips = sources // 2
    local_count = gate_w.shape[0]
    units = gate_w.shape[2]
    tok_rows = tok_in.shape[0]
    quarter = toks.shape[4]
    out_cols = down_w.shape[2]
    half_rows = tok_rows // 2
    cut = tok_rows * CUT_SIXTEENTHS // 16
    me = lax.axis_index("ep")
    tp = lax.axis_index("tp")
    z, core = me // 2, me % 2
    y, x = tp // 2, tp % 2
    tp_x = y * 2 + (1 - x)
    tp_y = (1 - y) * 2 + x
    mate = z * 2 + (1 - core)
    own_half = (x + y) % 2
    parts = 2 if cut < tok_rows else 1

    def partner(k):
        low = (z + k) % 2
        high = (z // 2 + k // 2) % 2
        return 2 * high + low

    def place(ep, column):
        return {"ep": ep, "tp": column}

    def remote(source, target, send, recv, where):
        return pltpu.make_async_remote_copy(
            src_ref=source,
            dst_ref=target,
            send_sem=send,
            recv_sem=recv,
            device_id=where,
            device_id_type=pl.DeviceIdType.MESH,
        )

    barrier = pltpu.get_barrier_semaphore()
    for d in range(1, sources):
        pl.semaphore_signal(
            barrier, inc=1, device_id=place((me + d) % sources, tp), device_id_type=pl.DeviceIdType.MESH
        )
    for column in (tp_x, tp_y):
        pl.semaphore_signal(
            barrier, inc=1, device_id=place(me, column), device_id_type=pl.DeviceIdType.MESH
        )

    tok_loads = [pltpu.make_async_copy(tokens_hbm, tok_in, tok_sem.at[0])]
    small = [
        pltpu.make_async_copy(gain_hbm, gain_in, local_sem.at[0]),
        pltpu.make_async_copy(ids_hbm, ids_in.at[me], local_sem.at[1]),
        pltpu.make_async_copy(mix_hbm, mix_in.at[me], local_sem.at[2]),
    ]
    tables = ((gate_hbm, gate_w), (up_hbm, up_w), (down_hbm, down_w))

    def load(w, n):
        hbm, vmem = tables[w]
        return pltpu.make_async_copy(hbm.at[n], vmem.at[n], weight_sem.at[w, n])

    for copy in small + tok_loads:
        copy.start()

    before = lax.broadcasted_iota(jnp.int32, (tok_rows, tok_rows), 0)
    after = lax.broadcasted_iota(jnp.int32, (tok_rows, tok_rows), 1)
    earlier[...] = (before < after).astype(jnp.float32).astype(jnp.bfloat16)

    def make_meta(source):
        ids, mix = ids_in[source], mix_in[source]
        named, scales = [], []
        for n in range(local_count):
            match = ids == me * local_count + n
            named.append(jnp.sum(match.astype(jnp.float32), axis=0, keepdims=True))
            scales.append(jnp.sum(jnp.where(match, mix, 0.0), axis=0, keepdims=True))
        pad = [jnp.zeros((1, tok_rows), jnp.float32)] * (8 - local_count)
        names = jnp.concatenate(named + pad, axis=0)
        slot = jnp.dot(names.astype(jnp.bfloat16), earlier[...], preferred_element_type=jnp.float32)
        slot = jnp.where(names > 0.0, slot, -1.0)
        meta[source, 0] = slot
        meta[source, 1] = jnp.concatenate(scales + pad, axis=0)

    for copy in small + tok_loads:
        copy.wait()
    load(0, 0).start()
    load(1, 0).start()
    band = 32

    @pl.loop(0, tok_rows // (2 * band))
    def _(p):
        @pl.when(p == 2)
        def _():
            for n in range(1, local_count):
                load(0, n).start()
                load(1, n).start()

        for n in range(2):
            at = pl.ds(pl.multiple_of((2 * p + n) * band, band), band)
            values = tok_in[at, :].astype(jnp.float32)
            centred = values - jnp.mean(values, axis=1, keepdims=True)
            row_var = jnp.mean(centred * centred, axis=1, keepdims=True)
            normal = (centred * lax.rsqrt(row_var + norm_eps) * gain_in[...]).astype(jnp.bfloat16)
            for q in range(4):
                toks[me, q // 2, q % 2, at, :] = normal[:, q * quarter : (q + 1) * quarter]

    def go(copy):
        copy.start()
        return copy

    def all_sent(piece, semaphore):
        remote(piece, piece, semaphore, back_recv.at[0], place(mate, tp)).wait_send()

    def all_here(piece, semaphore):
        remote(piece, piece, back_send.at[0], semaphore, place(mate, tp)).wait_recv()

    def line(chip, i, e, up):
        source = chip * 2 + i
        if e == 0:
            piece = toks.at[source, own_half, core]
        else:
            piece = toks.at[source, 1 - own_half, core, pl.ds(cut, tok_rows - cut)]
        return remote(
            piece,
            piece,
            line_send.at[up, e],
            line_recv.at[chip, i, e],
            place((z + 2 * up - 1) * 2 + core, tp),
        )

    def side(chip, i, along):
        piece = toks.at[chip * 2 + i, own_half, core, pl.ds(along * (cut // 2), cut // 2)]
        return remote(
            piece,
            piece,
            side_send.at[0],
            side_recv.at[chip, i],
            place(me, (tp_x, tp_y)[along]),
        )

    def to_mate(chip, i, m):
        source = chip * 2 + i
        piece = (
            toks.at[source, own_half, core],
            toks.at[source, 1 - own_half, core, pl.ds(cut, tok_rows - cut)] if parts > 1 else None,
            toks.at[source, 1 - own_half, core, pl.ds(0, cut)],
        )[m]
        return remote(
            piece, piece, mate_send.at[0], mate_recv.at[chip, i], place(mate, tp)
        )

    ends = ((1, z < chips - 1), (0, z > 0))

    def start_line(i):
        for e in range(parts):
            for up, there in ends:

                @pl.when(there)
                def _():
                    line(z, i, e, up).start()

    own_pieces = (
        toks.at[me, own_half, 1 - core],
        toks.at[me, 1 - own_half, 1 - core],
        toks.at[me, :, core],
    )
    own_copies = []
    metas = []

    def run_start():
        pl.semaphore_wait(barrier, sources + 1)
        for n, piece in enumerate(own_pieces):
            own_copies.append(
                go(remote(piece, piece, mate_send.at[0], own_recv.at[n], place(mate, tp)))
            )
        for d in range(1, sources):
            for n, table in enumerate((ids_in, mix_in)):
                metas.append(
                    go(
                        remote(
                            table.at[me],
                            table.at[me],
                            meta_send.at[n],
                            meta_recv.at[n],
                            place((me + d) % sources, tp),
                        )
                    )
                )
        @pl.when(core == 0)
        def _():
            start_line(0)

        make_meta(me)
        compute_act(0)
        send_act(0)
        for n in range(local_count):
            load(2, n).start()

    def run_line(distance, i, e):
        for up, chip in ((1, z - distance), (0, z + distance)):
            here = chip >= 0 if up else chip < chips
            ahead = z + 2 * up - 1

            @pl.when(here)
            def _():
                line(chip, i, e, up).wait_recv()

                @pl.when(ahead < chips if up else ahead >= 0)
                def _():
                    line(chip, i, e, up).start()

                if e == 0:
                    side(chip, i, 0).start()
                    side(chip, i, 1).start()
                to_mate(chip, i, e).start()


    def run_side(k, i):
        chip = partner(k)
        all_here(toks.at[chip * 2 + i, own_half, core, pl.ds(0, cut)], side_recv.at[chip, i])
        go(to_mate(chip, i, 2))

    def chosen(source):
        slots, scales = meta[source, 0], meta[source, 1]
        at = lax.broadcasted_iota(jnp.int32, (capacity, tok_rows), 0).astype(jnp.float32)
        hits = [at == slots[n : n + 1, :] for n in range(local_count)]
        ones = jnp.concatenate([h.astype(jnp.float32) for h in hits], axis=0)
        scale = jnp.concatenate(
            [
                jnp.sum(jnp.where(hits[n], scales[n : n + 1, :], 0.0), axis=1, keepdims=True)
                for n in range(local_count)
            ],
            axis=0,
        )
        return ones.astype(jnp.bfloat16), scale

    def source_of(s):
        if s == 0:
            return me
        if s == 1:
            return mate
        return partner(s // 2) * 2 + s % 2

    def compute_act(s):
        source = source_of(s)
        ones, _ = chosen(source)
        for q in range(4):
            got = jnp.dot(ones, toks[source, q // 2, q % 2], preferred_element_type=jnp.float32)
            got = got.astype(jnp.bfloat16)
            for n in range(local_count):
                rows[n, :, q * quarter : (q + 1) * quarter] = got[n * capacity : (n + 1) * capacity]

        @pl.loop(0, local_count)
        def _(n):
            if s == 0:
                load(0, n).wait()
                load(1, n).wait()
            block = rows[n]
            half = units // 2
            for part in range(2):
                cols = slice(part * half, (part + 1) * half)
                gate = jnp.dot(block, gate_w[n, :, cols], preferred_element_type=jnp.float32)
                up = jnp.dot(block, up_w[n, :, cols], preferred_element_type=jnp.float32)
                acts[s, tp, n, :, cols] = clamped_units(gate, up).astype(jnp.bfloat16)
            own_act(s, n, 0).start()
            if s == 0:

                @pl.when(n == 1 - core)
                def _():
                    own_copies[0].wait_recv()
                    own_copies[1].wait_recv()

                    @pl.when(core == 1)
                    def _():
                        start_line(0)

                    start_line(1)

    def own_act(s, n, along):
        piece = acts.at[s, tp, n]
        return remote(
            piece,
            piece,
            act_send.at[0],
            act_recv.at[s, 2 - (2 - along) * (1 - (n - along) * (n - along))],
            place(me, (tp_x, tp_y)[along]),
        )

    def passed_act(s, along):
        n = 1 - along
        piece = acts.at[s, (tp_y, tp_x)[along], n]
        return remote(
            piece,
            piece,
            act_send.at[0],
            act_recv.at[s, 2],
            place(me, (tp_x, tp_y)[along]),
        )

    def send_act(s):
        for n in reversed(range(local_count)):
            go(own_act(s, n, 1))

    def run_first(s):
        if metas:
            all_here(ids_in.at[pl.ds(0, sources - 1)], meta_recv.at[0])
            all_here(mix_in.at[pl.ds(0, sources - 1)], meta_recv.at[1])
            metas.clear()
        make_meta(source_of(s))
        if s == 1:
            own_copies[2].wait_recv()
        elif s > 1:
            chip = partner(s // 2)
            all_here(toks.at[chip * 2 + s % 2, :, core], mate_recv.at[chip, s % 2])
        compute_act(s)
        send_act(s)

    def pass_to_y(s):
        own_act(s, 0, 0).wait_recv()
        go(passed_act(s, 1))

    def pass_to_x(s):
        own_act(s, 1, 1).wait_recv()
        go(passed_act(s, 0))

    pairs = {}
    down_loads = [load(2, n) for n in range(local_count)]

    def run_second(s):
        while down_loads:
            down_loads.pop().wait()
        all_here(acts.at[s, pl.ds(0, 2)], act_recv.at[s, 2])

        @pl.loop(0, local_count)
        def _(n):
            total = jnp.zeros((capacity, out_cols), jnp.float32)
            for t in range(acts.shape[1]):
                total = total + jnp.dot(
                    acts[s, t, n],
                    down_w[n, t * units : (t + 1) * units, :],
                    preferred_element_type=jnp.float32,
                )
            weighted[n] = total

        ones, scale = chosen(source_of(s))
        value = jnp.concatenate([weighted[n] for n in range(local_count)], axis=0)
        value = (value * scale).astype(jnp.bfloat16)
        result = lax.dot_general(
            ones, value, (((0,), (0,)), ((), ())), preferred_element_type=jnp.float32
        )
        for h in range(2):
            combined[s, h] = result[h * half_rows : (h + 1) * half_rows]
        if s == 1:
            for h in range(2):
                pair_out[0, h] = combined[1, h].astype(jnp.bfloat16)
            piece, target = pair_out.at[0], pair_in.at[0]
        elif s > 1:
            pair_out[s // 2, s % 2] = combined[s, 1 - core].astype(jnp.bfloat16)
            piece, target = pair_out.at[s // 2, s % 2], pair_in.at[s // 2, s % 2]
        if s > 0:
            pairs[s] = go(remote(piece, target, pair_send.at[0], pair_recv.at[s], place(mate, tp)))

    def run_back(s):
        pairs[s].wait_recv()
        if s > 1:
            k, i = s // 2, s % 2
            both = combined[s, core] + pair_in[k, i].astype(jnp.float32)
            back_out[k, i] = both.astype(jnp.bfloat16)
            go(
                remote(
                    back_out.at[k, i],
                    back_in.at[z, core],
                    back_send.at[0],
                    back_recv.at[0],
                    place(partner(k) * 2 + i, tp),
                )
            )

    run_start()
    runs = {
        "L": run_line,
        "S": run_side,
        "F": run_first,
        "X": pass_to_y,
        "Y": pass_to_x,
        "D": run_second,
        "R": run_back,
    }
    for kind, *rest in STAGES:
        runs[kind](*rest)
    all_here(back_in.at[pl.ds(0, chips - 1)], back_recv.at[0])
    for h in range(2):
        result = combined[0, h] + pair_in[0, h].astype(jnp.float32)
        for d in range(1, chips):
            result = result + back_in[(z + d) % chips, h].astype(jnp.float32)
        out_ref[h * half_rows : (h + 1) * half_rows, :] = result.astype(out_ref.dtype)
    all_sent(ids_in.at[pl.ds(0, sources - 1)], meta_send.at[0])
    all_sent(mix_in.at[pl.ds(0, sources - 1)], meta_send.at[1])
    all_sent(toks.at[pl.ds(0, chips)], mate_send.at[0])
    all_sent(toks.at[pl.ds(0, 2 * chips - 2), 0, 0, pl.ds(0, cut)], side_send.at[0])
    all_sent(acts.at[pl.ds(0, 3 * sources // 4)], act_send.at[0])
    all_sent(pair_out, pair_send.at[0])
    all_sent(back_out.at[pl.ds(1, chips - 1)], back_send.at[0])
    for at in range(chips):

        @pl.when(z == at)
        def _():
            for up, chip_count in ((1, at + 1), (0, chips - at)):
                if chip_count == chips:
                    continue
                for e in range(parts):
                    first, size = ((0, tok_rows), (cut, tok_rows - cut))[e]
                    all_sent(
                        toks.at[pl.ds(0, 2 * chip_count), 0, 0, pl.ds(first, size)],
                        line_send.at[up, e],
                    )


def fused_per_device(tokens, norm_gain, route_ids, route_weights, w_gate, w_up, w_down):
    local_count, width, units = w_gate.shape
    out_cols = w_down.shape[2]
    sources = lax.axis_size("ep")
    tp_count = lax.axis_size("tp")
    experts = local_count * sources
    tok_rows, top_count = route_ids.shape
    capacity = 3 * tok_rows * top_count // (2 * experts)
    chips = sources // 2
    quarter = width // 4
    half_rows = tok_rows // 2
    dma = pltpu.SemaphoreType.DMA
    bf16 = jnp.bfloat16
    vmem = pl.BlockSpec(memory_space=pltpu.VMEM)
    hbm = pl.BlockSpec(memory_space=pltpu.HBM)
    return pl.pallas_call(
        functools.partial(layer_kernel, capacity),
        out_shape=pltpu.VMEM((tok_rows, out_cols), bf16),
        in_specs=[hbm] * 7,
        out_specs=vmem,
        scratch_shapes=[
            pltpu.VMEM(w_gate.shape, bf16),
            pltpu.VMEM(w_up.shape, bf16),
            pltpu.VMEM(w_down.shape, bf16),
            pltpu.VMEM(tokens.shape, bf16),
            pltpu.VMEM((1, width), jnp.float32),
            pltpu.VMEM((sources, top_count, tok_rows), jnp.int32),
            pltpu.VMEM((sources, top_count, tok_rows), jnp.float32),
            pltpu.VMEM((sources, 2, 2, tok_rows, quarter), bf16),
            pltpu.VMEM((sources, 2, 8, tok_rows), jnp.float32),
            pltpu.VMEM((tok_rows, tok_rows), bf16),
            pltpu.VMEM((local_count, capacity, width), bf16),
            pltpu.VMEM((sources, tp_count, local_count, capacity, units), bf16),
            pltpu.VMEM((local_count, capacity, out_cols), jnp.float32),
            pltpu.VMEM((sources, 2, half_rows, out_cols), jnp.float32),
            pltpu.VMEM((chips, 2, half_rows, out_cols), bf16),
            pltpu.VMEM((chips, 2, half_rows, out_cols), bf16),
            pltpu.VMEM((chips, 2, half_rows, out_cols), bf16),
            pltpu.VMEM((chips, 2, half_rows, out_cols), bf16),
            dma((3, local_count)),
            dma((1,)),
            dma((3,)),
            dma((2,)),
            dma((2,)),
            dma((3,)),
            dma((2, 2)),
            dma((chips, 2, 2)),
            dma((1,)),
            dma((chips, 2)),
            dma((1,)),
            dma((chips, 2)),
            dma((1,)),
            dma((sources, 3)),
            dma((1,)),
            dma((sources,)),
            dma((1,)),
            dma((1,)),
        ],
        compiler_params=pltpu.CompilerParams(
            collective_id=0, has_side_effects=True, vmem_limit_bytes=61 * 1024 * 1024
        ),
    )(tokens, norm_gain.reshape(1, width), route_ids.T, route_weights.T, w_gate, w_up, w_down)


def pick_plan(mesh):
    sources, tp_count = mesh.shape["ep"], mesh.shape["tp"]

    def body(tokens, norm_gain, route_ids, route_weights, w_gate, w_up, w_down):
        tok_rows, top_count = route_ids.shape
        experts = w_gate.shape[0] * sources
        capacity = 3 * tok_rows * top_count // (2 * experts)
        gathered = 2 * tokens.size * sources + 6 * w_gate.size
        fused = (
            tp_count == 4
            and sources == 8
            and capacity % 16 == 0
            and w_gate.shape[0] == 2
            and tok_rows % 128 == 0
            and tokens.shape[1] % 512 == 0
            and gathered < 32 * 1024 * 1024
        )
        run = fused_per_device if fused else per_device
        return run(tokens, norm_gain, route_ids, route_weights, w_gate, w_up, w_down)

    return body


def solution(mesh):
    return jax.shard_map(
        pick_plan(mesh),
        mesh=mesh,
        in_specs=(
            P("ep", None),
            P(),
            P("ep", None),
            P("ep", None),
            P("ep", None, "tp"),
            P("ep", None, "tp"),
            P("ep", None, "tp"),
        ),
        out_specs=P("ep", "tp"),
        check_vma=False,
    )
```

```python
import functools
import jax
import jax.numpy as jnp
from jax import lax
from jax.experimental import pallas as pl
from jax.experimental.pallas import tpu as pltpu
from jax.sharding import PartitionSpec as P

swiglu_limit = 7.0
swiglu_alpha = 1.702
norm_eps = 1e-05


def clamped_units(gate_pre, up_pre):
    capped = jnp.minimum(gate_pre, swiglu_limit)
    linear = jnp.clip(up_pre, -swiglu_limit, swiglu_limit)
    return capped * jax.nn.sigmoid(swiglu_alpha * capped) * (linear + 1.0)


def expert_work(outgoing, gate_weight, up_weight, down_weight):
    received = lax.all_to_all(outgoing, "ep", split_axis=1, concat_axis=1, tiled=True)
    local_count, sources, capacity, columns = received.shape
    row_count = sources * capacity
    row_block = received.reshape(local_count, row_count, columns)
    shard_piece = lax.all_gather(row_block, "tp", axis=2, tiled=True)
    gate_sum = jnp.einsum(
        "lrd,ldf->lrf", shard_piece, gate_weight, preferred_element_type=jnp.float32
    )
    up_sum = jnp.einsum("lrd,ldf->lrf", shard_piece, up_weight, preferred_element_type=jnp.float32)
    activation = clamped_units(gate_sum, up_sum).astype(jnp.bfloat16)
    out_cols = down_weight.shape[2]
    result = jnp.einsum(
        "lrf,lfd->lrd",
        lax.all_gather(activation, "tp", axis=2, tiled=True),
        down_weight,
        preferred_element_type=jnp.float32,
    )
    result = result.astype(jnp.bfloat16).reshape(local_count, sources, capacity, out_cols)
    return lax.all_to_all(result, "ep", split_axis=1, concat_axis=1, tiled=True)


def per_device(tokens, norm_gain, route_ids, route_weights, w_gate, w_up, w_down):
    local_count = w_gate.shape[0]
    sources = lax.axis_size("ep")
    tp_count = lax.axis_size("tp")
    width = tokens.shape[1]
    columns = width // tp_count
    experts = local_count * sources
    tok_rows, top_count = route_ids.shape
    capacity = 3 * tok_rows * top_count // (2 * experts)
    values = tokens.astype(jnp.float32)
    row_mean = jnp.mean(values, axis=1, keepdims=True)
    centred = values - row_mean
    row_var = jnp.mean(centred * centred, axis=1, keepdims=True)
    offset = lax.axis_index("tp") * columns
    own_cols = lax.dynamic_slice_in_dim(centred, offset, columns, 1)
    own_gain = lax.dynamic_slice_in_dim(norm_gain, offset, columns, 0)
    normed = (own_cols * lax.rsqrt(row_var + norm_eps) * own_gain).astype(jnp.bfloat16)
    flat_ids = route_ids.reshape(-1)
    matches = (flat_ids[:, None] == jnp.arange(experts, dtype=jnp.int32)[None, :]).astype(jnp.int32)
    earlier = jnp.cumsum(matches, axis=0) - matches
    slot_index = jnp.sum(earlier * matches, axis=1)
    position = (
        flat_ids % local_count * (sources * capacity)
        + flat_ids // local_count * capacity
        + slot_index
    )
    buffer_rows = local_count * sources * capacity
    placed = (
        position.reshape(tok_rows, top_count)[:, :, None]
        == jnp.arange(buffer_rows, dtype=jnp.int32)[None, None, :]
    )
    placement_matrix = jnp.any(placed, axis=1).astype(jnp.bfloat16)
    outgoing = jnp.einsum("tp,td->pd", placement_matrix, normed, preferred_element_type=jnp.float32)
    outgoing = outgoing.astype(jnp.bfloat16).reshape(local_count, sources, capacity, columns)
    returned = jnp.concatenate(
        [
            expert_work(
                outgoing[number : number + 1],
                w_gate[number : number + 1],
                w_up[number : number + 1],
                w_down[number : number + 1],
            )
            for number in range(local_count)
        ],
        axis=0,
    )
    flat_out = returned.reshape(buffer_rows, columns)
    picked = flat_out[position].reshape(tok_rows, top_count, columns).astype(jnp.float32)
    return jnp.sum(picked * route_weights[:, :, None], axis=1).astype(jnp.bfloat16)


CUT_SIXTEENTHS = 8
STAGES = (
    ("L", 1, 0, 0),
    ("F", 1),
    ("L", 1, 0, 1),
    ("S", 1, 0),
    ("L", 1, 1, 0),
    ("F", 2),
    ("L", 1, 1, 1),
    ("S", 1, 1),
    ("L", 2, 0, 0),
    ("X", 2),
    ("Y", 2),
    ("L", 2, 0, 1),
    ("F", 3),
    ("S", 2, 0),
    ("L", 2, 1, 0),
    ("F", 4),
    ("D", 2),
    ("X", 3),
    ("Y", 3),
    ("L", 2, 1, 1),
    ("Y", 4),
    ("S", 2, 1),
    ("X", 4),
    ("L", 3, 0, 0),
    ("F", 5),
    ("D", 3),
    ("D", 4),
    ("L", 3, 0, 1),
    ("S", 3, 0),
    ("L", 3, 1, 0),
    ("Y", 5),
    ("X", 5),
    ("R", 2),
    ("F", 6),
    ("L", 3, 1, 1),
    ("R", 4),
    ("S", 3, 1),
    ("D", 5),
    ("X", 6),
    ("Y", 6),
    ("F", 7),
    ("R", 5),
    ("D", 6),
    ("Y", 7),
    ("X", 7),
    ("X", 1),
    ("Y", 0),
    ("R", 6),
    ("R", 3),
    ("Y", 1),
    ("D", 7),
    ("X", 0),
    ("R", 7),
    ("D", 1),
    ("D", 0),
    ("R", 1),
)


def layer_kernel(
    capacity,
    tokens_hbm,
    gain_hbm,
    ids_hbm,
    mix_hbm,
    gate_hbm,
    up_hbm,
    down_hbm,
    out_ref,
    gate_w,
    up_w,
    down_w,
    tok_in,
    gain_in,
    ids_in,
    mix_in,
    toks,
    meta,
    earlier,
    rows,
    acts,
    weighted,
    combined,
    pair_out,
    pair_in,
    back_out,
    back_in,
    weight_sem,
    tok_sem,
    local_sem,
    meta_send,
    meta_recv,
    own_recv,
    line_send,
    line_recv,
    side_send,
    side_recv,
    mate_send,
    mate_recv,
    act_send,
    act_recv,
    pair_send,
    pair_recv,
    back_send,
    back_recv,
):
    sources = toks.shape[0]
    chips = sources // 2
    local_count = gate_w.shape[0]
    units = gate_w.shape[2]
    tok_rows = tok_in.shape[0]
    quarter = toks.shape[4]
    out_cols = down_w.shape[2]
    half_rows = tok_rows // 2
    cut = tok_rows * CUT_SIXTEENTHS // 16
    me = lax.axis_index("ep")
    tp = lax.axis_index("tp")
    z, core = me // 2, me % 2
    y, x = tp // 2, tp % 2
    tp_x = y * 2 + (1 - x)
    tp_y = (1 - y) * 2 + x
    mate = z * 2 + (1 - core)
    own_half = (x + y) % 2
    parts = 2 if cut < tok_rows else 1

    def partner(k):
        low = (z + k) % 2
        high = (z // 2 + k // 2) % 2
        return 2 * high + low

    outer = (z + 1) % chips < 2
    inner = (z + 1) % chips >= 2

    def place(ep, column):
        return {"ep": ep, "tp": column}

    def remote(source, target, send, recv, where):
        return pltpu.make_async_remote_copy(
            src_ref=source,
            dst_ref=target,
            send_sem=send,
            recv_sem=recv,
            device_id=where,
            device_id_type=pl.DeviceIdType.MESH,
        )

    barrier = pltpu.get_barrier_semaphore()
    for d in range(1, sources):
        pl.semaphore_signal(
            barrier, inc=1, device_id=place((me + d) % sources, tp), device_id_type=pl.DeviceIdType.MESH
        )
    for column in (tp_x, tp_y):
        pl.semaphore_signal(
            barrier, inc=1, device_id=place(me, column), device_id_type=pl.DeviceIdType.MESH
        )

    tok_loads = [pltpu.make_async_copy(tokens_hbm, tok_in, tok_sem.at[0])]
    small = [
        pltpu.make_async_copy(gain_hbm, gain_in, local_sem.at[0]),
        pltpu.make_async_copy(ids_hbm, ids_in.at[me], local_sem.at[1]),
        pltpu.make_async_copy(mix_hbm, mix_in.at[me], local_sem.at[2]),
    ]
    tables = ((gate_hbm, gate_w), (up_hbm, up_w), (down_hbm, down_w))

    def load(w, n):
        hbm, vmem = tables[w]
        return pltpu.make_async_copy(hbm.at[n], vmem.at[n], weight_sem.at[w, n])

    for copy in small + tok_loads:
        copy.start()

    before = lax.broadcasted_iota(jnp.int32, (tok_rows, tok_rows), 0)
    after = lax.broadcasted_iota(jnp.int32, (tok_rows, tok_rows), 1)
    earlier[...] = (before < after).astype(jnp.float32).astype(jnp.bfloat16)

    def make_meta(source):
        ids, mix = ids_in[source], mix_in[source]
        named, scales = [], []
        for n in range(local_count):
            match = ids == me * local_count + n
            named.append(jnp.sum(match.astype(jnp.float32), axis=0, keepdims=True))
            scales.append(jnp.sum(jnp.where(match, mix, 0.0), axis=0, keepdims=True))
        pad = [jnp.zeros((1, tok_rows), jnp.float32)] * (8 - local_count)
        names = jnp.concatenate(named + pad, axis=0)
        slot = jnp.dot(names.astype(jnp.bfloat16), earlier[...], preferred_element_type=jnp.float32)
        slot = jnp.where(names > 0.0, slot, -1.0)
        meta[source, 0] = slot
        meta[source, 1] = jnp.concatenate(scales + pad, axis=0)

    for copy in small + tok_loads:
        copy.wait()
    load(0, 0).start()
    load(1, 0).start()
    band = 32

    @pl.loop(0, tok_rows // (2 * band))
    def _(p):
        @pl.when(p == 2)
        def _():
            for n in range(1, local_count):
                load(0, n).start()
                load(1, n).start()

        for n in range(2):
            at = pl.ds(pl.multiple_of((2 * p + n) * band, band), band)
            values = tok_in[at, :].astype(jnp.float32)
            centred = values - jnp.mean(values, axis=1, keepdims=True)
            row_var = jnp.mean(centred * centred, axis=1, keepdims=True)
            normal = (centred * lax.rsqrt(row_var + norm_eps) * gain_in[...]).astype(jnp.bfloat16)
            for q in range(4):
                toks[me, q // 2, q % 2, at, :] = normal[:, q * quarter : (q + 1) * quarter]

    def go(copy):
        copy.start()
        return copy

    def all_sent(piece, semaphore):
        remote(piece, piece, semaphore, back_recv.at[0], place(mate, tp)).wait_send()

    def all_here(piece, semaphore):
        remote(piece, piece, back_send.at[0], semaphore, place(mate, tp)).wait_recv()

    def line(chip, i, e, up):
        source = chip * 2 + i
        if e == 0:
            piece = toks.at[source, own_half, core]
        else:
            piece = toks.at[source, 1 - own_half, core, pl.ds(cut, tok_rows - cut)]
        return remote(
            piece,
            piece,
            line_send.at[up, e],
            line_recv.at[chip, i, e],
            place((z + 2 * up - 1) * 2 + core, tp),
        )

    def side(chip, i, near, along):
        size = (tok_rows if near else cut) // 2
        piece = toks.at[chip * 2 + i, own_half, core, pl.ds(along * size, size)]
        return remote(
            piece,
            piece,
            side_send.at[near],
            side_recv.at[chip, i],
            place(me, (tp_x, tp_y)[along]),
        )

    def to_mate(chip, i, m):
        source = chip * 2 + i
        piece = (
            toks.at[source, own_half, core],
            toks.at[source, 1 - own_half, core, pl.ds(cut, tok_rows - cut)] if parts > 1 else None,
            toks.at[source, 1 - own_half, core, pl.ds(0, cut)],
            toks.at[source, 1 - own_half, core],
        )[m]
        return remote(
            piece, piece, mate_send.at[0], mate_recv.at[chip, i], place(mate, tp)
        )

    ends = ((1, z < chips - 1), (0, z > 0))

    def start_line(i):
        for up, there in ends:

            @pl.when(there)
            def _():
                line(z, i, 0, up).start()

            if parts > 1:

                @pl.when(z < chips - 2 if up else z > 1)
                def _():
                    line(z, i, 1, up).start()

    own_pieces = (
        toks.at[me, own_half, 1 - core],
        toks.at[me, 1 - own_half, 1 - core],
        toks.at[me, :, core],
    )
    own_copies = []
    metas = []

    def run_start():
        @pl.when(z == 0)
        def _():
            make_meta(me)
            compute_act(0, True)

        pl.semaphore_wait(barrier, sources + 1)
        for n, piece in enumerate(own_pieces):
            own_copies.append(
                go(remote(piece, piece, mate_send.at[0], own_recv.at[n], place(mate, tp)))
            )
        for d in range(1, sources):
            for n, table in enumerate((ids_in, mix_in)):
                metas.append(
                    go(
                        remote(
                            table.at[me],
                            table.at[me],
                            meta_send.at[n],
                            meta_recv.at[n],
                            place((me + d) % sources, tp),
                        )
                    )
                )
        @pl.when(core == 0)
        def _():
            start_line(0)

        @pl.when(z == 0)
        def _():
            for n in range(local_count):
                own_act(0, n, 0).start()
            send_act(0)
            start_rest()

        @pl.when(z > 0)
        def _():
            make_meta(me)
            compute_act(0)
            send_act(0)

        for n in range(local_count):
            load(2, n).start()

    def run_line(distance, i, e):
        for up, chip in ((1, z - distance), (0, z + distance)):
            here = chip >= 0 if up else chip < chips
            ahead = z + 2 * up - 1
            if distance == 1 and e == 1:
                here = jnp.logical_and(here, inner)

            @pl.when(here)
            def _():
                line(chip, i, e, up).wait_recv()

                @pl.when(ahead < chips if up else ahead >= 0)
                def _():
                    line(chip, i, e, up).start()

                if e == 0 and distance > 1:
                    for along in range(2):
                        side(chip, i, 0, along).start()
                to_mate(chip, i, e).start()

            if e == 0 and distance == 1:
                for near, which in ((1, outer), (0, inner)):

                    @pl.when(jnp.logical_and(here, which))
                    def _():
                        for along in range(2):
                            side(chip, i, near, along).start()

    def run_side(distance, i):
        for up, chip in ((1, z - distance), (0, z + distance)):
            here = chip >= 0 if up else chip < chips

            def arrived(size, m):
                all_here(
                    toks.at[chip * 2 + i, own_half, core, pl.ds(0, size)], side_recv.at[chip, i]
                )
                to_mate(chip, i, m).start()

            if distance > 1:

                @pl.when(here)
                def _():
                    arrived(cut, 2)
            else:

                @pl.when(jnp.logical_and(here, outer))
                def _():
                    arrived(tok_rows, 3)

                @pl.when(jnp.logical_and(here, inner))
                def _():
                    arrived(cut, 2)

    def chosen(source):
        slots, scales = meta[source, 0], meta[source, 1]
        at = lax.broadcasted_iota(jnp.int32, (capacity, tok_rows), 0).astype(jnp.float32)
        hits = [at == slots[n : n + 1, :] for n in range(local_count)]
        ones = jnp.concatenate([h.astype(jnp.float32) for h in hits], axis=0)
        scale = jnp.concatenate(
            [
                jnp.sum(jnp.where(hits[n], scales[n : n + 1, :], 0.0), axis=1, keepdims=True)
                for n in range(local_count)
            ],
            axis=0,
        )
        return ones.astype(jnp.bfloat16), scale

    def source_of(s):
        if s == 0:
            return me
        if s == 1:
            return mate
        return partner(s // 2) * 2 + s % 2

    def start_rest():
        own_copies[0].wait_recv()
        own_copies[1].wait_recv()

        @pl.when(core == 1)
        def _():
            start_line(0)

        start_line(1)

    def compute_act(s, hold=False):
        source = source_of(s)
        ones, _ = chosen(source)
        for q in range(4):
            got = jnp.dot(ones, toks[source, q // 2, q % 2], preferred_element_type=jnp.float32)
            got = got.astype(jnp.bfloat16)
            for n in range(local_count):
                rows[n, :, q * quarter : (q + 1) * quarter] = got[n * capacity : (n + 1) * capacity]

        @pl.loop(0, local_count)
        def _(n):
            if s == 0:
                load(0, n).wait()
                load(1, n).wait()
            block = rows[n]
            half = units // 2
            for part in range(2):
                cols = slice(part * half, (part + 1) * half)
                gate = jnp.dot(block, gate_w[n, :, cols], preferred_element_type=jnp.float32)
                up = jnp.dot(block, up_w[n, :, cols], preferred_element_type=jnp.float32)
                acts[s, tp, n, :, cols] = clamped_units(gate, up).astype(jnp.bfloat16)
            if not hold:
                own_act(s, n, 0).start()
            if s == 0 and not hold:

                @pl.when(n == 1 - core)
                def _():
                    start_rest()

    def own_act(s, n, along):
        piece = acts.at[s, tp, n]
        return remote(
            piece,
            piece,
            act_send.at[0],
            act_recv.at[s, 2 - (2 - along) * (1 - (n - along) * (n - along))],
            place(me, (tp_x, tp_y)[along]),
        )

    def passed_act(s, along):
        n = 1 - along
        piece = acts.at[s, (tp_y, tp_x)[along], n]
        return remote(
            piece,
            piece,
            act_send.at[0],
            act_recv.at[s, 2],
            place(me, (tp_x, tp_y)[along]),
        )

    def send_act(s):
        for n in reversed(range(local_count)):
            go(own_act(s, n, 1))

    def run_first(s):
        if metas:
            all_here(ids_in.at[pl.ds(0, sources - 1)], meta_recv.at[0])
            all_here(mix_in.at[pl.ds(0, sources - 1)], meta_recv.at[1])
            metas.clear()
        make_meta(source_of(s))
        if s == 1:
            own_copies[2].wait_recv()
        elif s > 1:
            chip = partner(s // 2)
            all_here(toks.at[chip * 2 + s % 2, :, core], mate_recv.at[chip, s % 2])
        compute_act(s)
        send_act(s)

    def pass_to_y(s):
        own_act(s, 0, 0).wait_recv()
        go(passed_act(s, 1))

    def pass_to_x(s):
        own_act(s, 1, 1).wait_recv()
        go(passed_act(s, 0))

    pairs = {}
    down_loads = [load(2, n) for n in range(local_count)]

    def run_second(s):
        while down_loads:
            down_loads.pop().wait()
        all_here(acts.at[s, pl.ds(0, 2)], act_recv.at[s, 2])

        @pl.loop(0, local_count)
        def _(n):
            total = jnp.zeros((capacity, out_cols), jnp.float32)
            for t in range(acts.shape[1]):
                total = total + jnp.dot(
                    acts[s, t, n],
                    down_w[n, t * units : (t + 1) * units, :],
                    preferred_element_type=jnp.float32,
                )
            weighted[n] = total

        ones, scale = chosen(source_of(s))
        value = jnp.concatenate([weighted[n] for n in range(local_count)], axis=0)
        value = (value * scale).astype(jnp.bfloat16)
        result = lax.dot_general(
            ones, value, (((0,), (0,)), ((), ())), preferred_element_type=jnp.float32
        )
        for h in range(2):
            combined[s, h] = result[h * half_rows : (h + 1) * half_rows]
        if s == 1:
            for h in range(2):
                pair_out[0, h] = combined[1, h].astype(jnp.bfloat16)
            piece, target = pair_out.at[0], pair_in.at[0]
        elif s > 1:
            pair_out[s // 2, s % 2] = combined[s, 1 - core].astype(jnp.bfloat16)
            piece, target = pair_out.at[s // 2, s % 2], pair_in.at[s // 2, s % 2]
        if s > 0:
            pairs[s] = go(remote(piece, target, pair_send.at[0], pair_recv.at[s], place(mate, tp)))

    def run_back(s):
        pairs[s].wait_recv()
        if s > 1:
            k, i = s // 2, s % 2
            both = combined[s, core] + pair_in[k, i].astype(jnp.float32)
            back_out[k, i] = both.astype(jnp.bfloat16)
            go(
                remote(
                    back_out.at[k, i],
                    back_in.at[z, core],
                    back_send.at[0],
                    back_recv.at[0],
                    place(partner(k) * 2 + i, tp),
                )
            )

    run_start()
    runs = {
        "L": run_line,
        "S": run_side,
        "F": run_first,
        "X": pass_to_y,
        "Y": pass_to_x,
        "D": run_second,
        "R": run_back,
    }
    for kind, *rest in STAGES:
        runs[kind](*rest)
    all_here(back_in.at[pl.ds(0, chips - 1)], back_recv.at[0])
    for h in range(2):
        result = combined[0, h] + pair_in[0, h].astype(jnp.float32)
        for d in range(1, chips):
            result = result + back_in[(z + d) % chips, h].astype(jnp.float32)
        out_ref[h * half_rows : (h + 1) * half_rows, :] = result.astype(out_ref.dtype)
    all_sent(ids_in.at[pl.ds(0, sources - 1)], meta_send.at[0])
    all_sent(mix_in.at[pl.ds(0, sources - 1)], meta_send.at[1])
    all_sent(toks.at[pl.ds(0, chips)], mate_send.at[0])
    all_sent(acts.at[pl.ds(0, 3 * sources // 4)], act_send.at[0])
    all_sent(pair_out, pair_send.at[0])
    all_sent(back_out.at[pl.ds(1, chips - 1)], back_send.at[0])
    for at in range(chips):

        @pl.when(z == at)
        def _():
            edge = at in (0, chips - 1)
            if edge:
                all_sent(toks.at[pl.ds(0, 2), 0, 0], side_send.at[1])
            far = 2 * (chips - 1 - edge)
            all_sent(toks.at[pl.ds(0, far), 0, 0, pl.ds(0, cut)], side_send.at[0])
            for up, behind in ((1, at), (0, chips - 1 - at)):
                if behind == chips - 1:
                    continue
                all_sent(toks.at[pl.ds(0, 2 * behind + 2), 0, 0], line_send.at[up, 0])
                extra = behind + int(behind < chips - 2)
                if parts > 1:
                    all_sent(
                        toks.at[pl.ds(0, 2 * extra), 0, 0, pl.ds(cut, tok_rows - cut)],
                        line_send.at[up, 1],
                    )


def fused_per_device(tokens, norm_gain, route_ids, route_weights, w_gate, w_up, w_down):
    local_count, width, units = w_gate.shape
    out_cols = w_down.shape[2]
    sources = lax.axis_size("ep")
    tp_count = lax.axis_size("tp")
    experts = local_count * sources
    tok_rows, top_count = route_ids.shape
    capacity = 3 * tok_rows * top_count // (2 * experts)
    chips = sources // 2
    quarter = width // 4
    half_rows = tok_rows // 2
    dma = pltpu.SemaphoreType.DMA
    bf16 = jnp.bfloat16
    vmem = pl.BlockSpec(memory_space=pltpu.VMEM)
    hbm = pl.BlockSpec(memory_space=pltpu.HBM)
    return pl.pallas_call(
        functools.partial(layer_kernel, capacity),
        out_shape=pltpu.VMEM((tok_rows, out_cols), bf16),
        in_specs=[hbm] * 7,
        out_specs=vmem,
        scratch_shapes=[
            pltpu.VMEM(w_gate.shape, bf16),
            pltpu.VMEM(w_up.shape, bf16),
            pltpu.VMEM(w_down.shape, bf16),
            pltpu.VMEM(tokens.shape, bf16),
            pltpu.VMEM((1, width), jnp.float32),
            pltpu.VMEM((sources, top_count, tok_rows), jnp.int32),
            pltpu.VMEM((sources, top_count, tok_rows), jnp.float32),
            pltpu.VMEM((sources, 2, 2, tok_rows, quarter), bf16),
            pltpu.VMEM((sources, 2, 8, tok_rows), jnp.float32),
            pltpu.VMEM((tok_rows, tok_rows), bf16),
            pltpu.VMEM((local_count, capacity, width), bf16),
            pltpu.VMEM((sources, tp_count, local_count, capacity, units), bf16),
            pltpu.VMEM((local_count, capacity, out_cols), jnp.float32),
            pltpu.VMEM((sources, 2, half_rows, out_cols), jnp.float32),
            pltpu.VMEM((chips, 2, half_rows, out_cols), bf16),
            pltpu.VMEM((chips, 2, half_rows, out_cols), bf16),
            pltpu.VMEM((chips, 2, half_rows, out_cols), bf16),
            pltpu.VMEM((chips, 2, half_rows, out_cols), bf16),
            dma((3, local_count)),
            dma((1,)),
            dma((3,)),
            dma((2,)),
            dma((2,)),
            dma((3,)),
            dma((2, 2)),
            dma((chips, 2, 2)),
            dma((2,)),
            dma((chips, 2)),
            dma((1,)),
            dma((chips, 2)),
            dma((1,)),
            dma((sources, 3)),
            dma((1,)),
            dma((sources,)),
            dma((1,)),
            dma((1,)),
        ],
        compiler_params=pltpu.CompilerParams(
            collective_id=0, has_side_effects=True, vmem_limit_bytes=61 * 1024 * 1024
        ),
    )(tokens, norm_gain.reshape(1, width), route_ids.T, route_weights.T, w_gate, w_up, w_down)


def pick_plan(mesh):
    sources, tp_count = mesh.shape["ep"], mesh.shape["tp"]

    def body(tokens, norm_gain, route_ids, route_weights, w_gate, w_up, w_down):
        tok_rows, top_count = route_ids.shape
        experts = w_gate.shape[0] * sources
        capacity = 3 * tok_rows * top_count // (2 * experts)
        gathered = 2 * tokens.size * sources + 6 * w_gate.size
        fused = (
            tp_count == 4
            and sources == 8
            and capacity % 16 == 0
            and w_gate.shape[0] == 2
            and tok_rows % 128 == 0
            and tokens.shape[1] % 512 == 0
            and gathered < 32 * 1024 * 1024
        )
        run = fused_per_device if fused else per_device
        return run(tokens, norm_gain, route_ids, route_weights, w_gate, w_up, w_down)

    return body


def solution(mesh):
    return jax.shard_map(
        pick_plan(mesh),
        mesh=mesh,
        in_specs=(
            P("ep", None),
            P(),
            P("ep", None),
            P("ep", None),
            P("ep", None, "tp"),
            P("ep", None, "tp"),
            P("ep", None, "tp"),
        ),
        out_specs=P("ep", "tp"),
        check_vma=False,
    )
```
